32 devices in a mesh: ep: 16 (over z, y, x), tp: 2 (over core).
Axes of the slice: x: 2, y: 2, z: 4, core: 2. Of those that a mesh axis runs over, the one named last changes fastest.
Arguments:
- tokens: bfloat16 [112, 2304], P('ep'), may hold values from -6 to 6
- attn_gain: bfloat16 [2304], replicated, may hold values from 0.099609375 to 1.8984375
- query_weight: bfloat16 [2304, 2048], P(None, 'tp'), may hold values from -0.125 to 0.125
- key_weight: bfloat16 [2304, 2048], P(None, 'tp'), may hold values from -0.125 to 0.125
- value_weight: bfloat16 [2304, 2048], P(None, 'tp'), may hold values from -0.125 to 0.125
- out_weight: bfloat16 [2304, 2048], P(None, 'tp'), may hold values from -0.125 to 0.125
- lambdas: float32 [16], P('tp'), may hold values from 0.3 to 0.8
- head_gain: bfloat16 [128], replicated, may hold values from 0.099609375 to 1.8984375
- cache_keys: bfloat16 [112, 1024, 16, 128], P('ep', None, 'tp'), may hold values from -1500 to 1500
- cache_values: bfloat16 [112, 1024, 16, 128], P('ep', None, 'tp'), may hold values from -6 to 6
- lengths: int32 [112], P('ep'), may hold values from 2 to 1024, as said below
- moe_gain: bfloat16 [2304], replicated, may hold values from 0.099609375 to 1.8984375
- gate_weight: bfloat16 [16, 2304, 1024], P('ep', None, 'tp'), may hold values from -0.125 to 0.125
- up_weight: bfloat16 [16, 2304, 1024], P('ep', None, 'tp'), may hold values from -0.125 to 0.125
- down_weight: bfloat16 [16, 1024, 2304], P('ep', 'tp'), may hold values from -0.1875 to 0.1875
- shared_gate: bfloat16 [2304, 1024], P(None, 'tp'), may hold values from -0.125 to 0.125
- shared_up: bfloat16 [2304, 1024], P(None, 'tp'), may hold values from -0.125 to 0.125
- shared_down: bfloat16 [1024, 2304], P('tp'), may hold values from -0.1875 to 0.1875
- expert_ids: int32 [112, 6], P('ep'), may hold values from 0 to 15, all different within a row; in each aligned block of 7 rows (0 to 6, 7 to 13, ...) at most 5 rows name the same one
- expert_weights: float32 [112, 6], P('ep'), may hold values from 0.2 to 1
Outputs:
- result: bfloat16 [112, 2304], P('ep', 'tp')
The draws below stay inside these ranges and needn't reach their ends.
Inputs may be any that keep to these rules, and one draw needn't show every extreme that they name: `expert_ids`: each row names 6 different experts. Among the rows of one device (aligned blocks of 7 rows) no expert is named by more than 5 rows, a bound that some block reaches. `lengths`: some sequence has 1024 cached positions.
All inputs are finite; a program needn't handle non-finite values.
Results may differ from the reference program's by a relative error of at most 0.02.
Values may be sent and summed in bfloat16 or wider, within the bound.
No kernel may reach another device: no remote copies, remote signals or barrier semaphores. Data moves between devices by JAX's collectives and lax.ppermute only.
A program may use at most 128 MiB of HBM per device.

```python
import math
import jax
import jax.numpy as jnp
import numpy as np
from jax import lax

D = 2304
HEADS = 16
HD = 64
VD = 128
EW = 1024
SW = 1024
TOP = 6
SEQ_DEV = 7
CACHE_LEN = 1024
SEQS = 112
EXPERTS = 16
CAP = 5
N_EP = 16
N_TP = 2


def draw_cache_keys(key, part):
    base_draw = jnp.clip(jax.random.normal(key, (SEQS, CACHE_LEN, HEADS, 2 * HD), jnp.float32), -8.0, 8.0) * 1.75
    return base_draw.astype(jnp.bfloat16)


def draw_lengths(key, part):
    key_one, key_two = jax.random.split(jax.random.fold_in(key, 3))
    group_count = SEQS // SEQ_DEV
    group_top = jax.random.randint(key_one, (group_count, 1), CACHE_LEN // 4, CACHE_LEN + 1)
    drawn = jax.random.randint(key_two, (group_count, SEQ_DEV), 2, group_top + 1)
    drawn = drawn.reshape(-1).astype(jnp.int32)
    return drawn.at[0].set(CACHE_LEN)


def steps_of(rng, dims, pieces, least, high):
    def one(axis_at, blocks):
        heights = jax.random.uniform(jax.random.fold_in(jax.random.fold_in(rng, 6), axis_at), (blocks,), jnp.float32, least / len(pieces), high / len(pieces))
        return jnp.repeat(jnp.exp(heights), dims[axis_at] // blocks).reshape((-1,) + (1,) * (len(dims) - axis_at - 1))

    level = one(*pieces[0])
    for cut in pieces[1:]:
        level = level * one(*cut)
    return level


def routed_block(key, own, number, rows, count, top, bound, lean):
    order = jax.random.permutation(key, count)
    heavy_load, usual = shares(count, rows * top, bound, lean, True), shares(count, rows * top, bound, lean, False)
    places = jnp.arange(count)

    def named(tallies, offset_by):
        used = int((tallies > 0).sum())
        fixed = max(1, used // 4)
        moved = fixed + (places - fixed + offset_by * (used - fixed)) % max(1, count - fixed)
        return jnp.zeros((count,), jnp.int32).at[order[jnp.where(places < fixed, places, moved)]].set(jnp.asarray(tallies, jnp.int32))

    tallies = jnp.where(number % 4 == 0, named(heavy_load, number // 4), named(usual, number - number // 4 - 1))
    mixed = jax.random.permutation(jax.random.fold_in(own, 3), count)
    source_of, receiver = mixed[0:count // 2 * 2:2], mixed[1:count // 2 * 2:2]
    margin = jnp.minimum(tallies[source_of] - 1, bound - tallies[receiver]) // 2
    margin = jnp.where((source_of == order[0]) | (receiver == order[0]) | (tallies[receiver] == 0), 0, jnp.maximum(margin, 0))
    moved = jax.random.randint(jax.random.fold_in(own, 4), (count // 2,), 0, 1 << 20) % (margin + 1)
    tallies = tallies.at[source_of].add(-moved).at[receiver].add(moved)
    items = jnp.searchsorted(jnp.cumsum(tallies), jnp.arange(rows * top), side="right").astype(jnp.int32)
    grid = items.reshape(top, rows).T
    grid = grid[jax.random.permutation(jax.random.fold_in(own, 1), rows)]
    offset_by = jax.random.randint(jax.random.fold_in(own, 2), (rows, 1), 0, top)
    return jnp.take_along_axis(grid, (jnp.arange(top)[None, :] + offset_by) % top, axis=1)


def shares(count, total, limit, slope, full):
    portions = [(1 << 20) // math.isqrt(rank ** slope) + 1 for rank in range(1, count + 1)]
    largest = limit if full else min(limit, max(-(-total // count), total * portions[0] // sum(portions)))
    least = 1 if total - largest >= count - 1 else 0
    counts, spare = [largest] + [least] * (count - 1), total - largest - least * (count - 1)
    while spare > 0:
        candidates = [i for i in range(1, count) if counts[i] < largest] or [i for i in range(1, count) if counts[i] < limit]
        pool, remaining = sum([portions[i] for i in candidates]), spare
        for i in candidates:
            extra = min(limit - counts[i], max(1, remaining * portions[i] // pool), spare)
            counts[i] = counts[i] + extra
            spare = spare - extra
    return np.array(counts)


def bell_draw(rng, dims, width, limit, pieces=(), kind=jnp.bfloat16):
    result = width * jax.random.normal(rng, dims, jnp.float32)
    if pieces:
        result = result * steps_of(rng, dims, pieces, -0.22, 0.18)
    return jnp.clip(result, -limit, limit).astype(kind)


def setup_inputs(seed: int = 0) -> dict:
    splits = jax.random.split(jax.random.key(seed), 21)
    tokens = bell_draw(splits[0], (SEQS, D), 1.0, 6.0, ((0, 16),))
    attn_gain = jnp.clip(1.0 + 0.18 * jax.random.normal(splits[1], (D,), jnp.float32), 0.099609375, 1.8984375).astype(jnp.bfloat16)
    query_weight = bell_draw(splits[2], (D, HEADS * 2 * HD), D ** -0.5, 0.125, ((1, 2),))
    key_weight = bell_draw(splits[3], (D, HEADS * 2 * HD), D ** -0.5, 0.125, ((1, 2),))
    value_weight = bell_draw(splits[4], (D, HEADS * VD), D ** -0.5, 0.125, ((1, 2),))
    out_weight = bell_draw(splits[5], (D, HEADS * VD), (HEADS * VD) ** -0.5, 0.125, ((1, 2),))
    lambdas = jnp.clip(0.3 + 0.5 * jax.random.uniform(splits[6], (HEADS,), jnp.float32) ** steps_of(splits[6], (HEADS,), ((0, 2),), -0.2, 0.2), 0.3, 0.8)
    head_gain = jnp.clip(1.0 + 0.18 * jax.random.normal(splits[7], (VD,), jnp.float32), 0.099609375, 1.8984375).astype(jnp.bfloat16)
    cache_keys = draw_cache_keys(jax.random.fold_in(splits[20], 71), 0)
    cache_values = bell_draw(splits[9], (SEQS, CACHE_LEN, HEADS, VD), 1.0, 6.0, ((0, 16), (2, 2)))
    lengths = draw_lengths(jax.random.fold_in(splits[20], 71), 0)
    moe_gain = jnp.clip(1.0 + 0.18 * jax.random.normal(splits[11], (D,), jnp.float32), 0.099609375, 1.8984375).astype(jnp.bfloat16)
    gate_weight = bell_draw(splits[12], (EXPERTS, D, EW), D ** -0.5, 0.125, ((0, 16), (2, 2)))
    up_weight = bell_draw(splits[13], (EXPERTS, D, EW), D ** -0.5, 0.125, ((0, 16), (2, 2)))
    down_weight = bell_draw(splits[14], (EXPERTS, EW, D), EW ** -0.5, 0.1875, ((0, 16), (1, 2)))
    shared_gate = bell_draw(splits[15], (D, SW), D ** -0.5, 0.125, ((1, 2),))
    shared_up = bell_draw(splits[16], (D, SW), D ** -0.5, 0.125, ((1, 2),))
    shared_down = bell_draw(splits[17], (SW, D), SW ** -0.5, 0.1875, ((0, 2),))
    expert_ids_keys = jax.random.split(jax.random.fold_in(splits[18], 1), SEQS // SEQ_DEV)
    expert_ids_turns = jax.random.permutation(jax.random.fold_in(splits[18], 3), SEQS // SEQ_DEV)
    expert_ids = jax.vmap(lambda own, number: routed_block(jax.random.fold_in(splits[18], 2), own, number, SEQ_DEV, EXPERTS, TOP, CAP, 2))(expert_ids_keys, expert_ids_turns).reshape((SEQS, TOP))
    expert_weights = jnp.clip(0.2 + 0.8 * jax.random.uniform(splits[19], (SEQS, TOP), jnp.float32) ** steps_of(splits[19], (SEQS, TOP), ((0, 16),), -0.2, 0.2), 0.2, 1.0)
    return {"tokens": tokens, "attn_gain": attn_gain, "query_weight": query_weight, "key_weight": key_weight, "value_weight": value_weight, "out_weight": out_weight, "lambdas": lambdas, "head_gain": head_gain, "cache_keys": cache_keys, "cache_values": cache_values, "lengths": lengths, "moe_gain": moe_gain, "gate_weight": gate_weight, "up_weight": up_weight, "down_weight": down_weight, "shared_gate": shared_gate, "shared_up": shared_up, "shared_down": shared_down, "expert_ids": expert_ids, "expert_weights": expert_weights}


epsilon = 1e-06

def rms_scale(values, gain):
    wide = values.astype(jnp.float32)
    return wide * lax.rsqrt(lax.optimization_barrier(jnp.mean(wide * wide, axis=-1, keepdims=True)) + epsilon) * gain.astype(jnp.float32)

def rounded(values):
    return lax.optimization_barrier(values.astype(jnp.bfloat16)).astype(jnp.float32)

def attend_group(blocks, lambdas):
    query_rows, key_rows, value_rows, past_keys, past_values, seq_lengths = blocks
    seq_count = query_rows.shape[0]
    head_dim = past_keys.shape[-1] // 2
    score_scale = head_dim ** (-0.5)
    queries = query_rows.astype(jnp.float32).reshape(seq_count, HEADS, 2, head_dim)
    new_keys = key_rows.astype(jnp.float32).reshape(seq_count, HEADS, 2, head_dim)
    new_values = value_rows.astype(jnp.float32).reshape(seq_count, HEADS, 2 * head_dim)
    cache_rows = past_keys.astype(jnp.float32).reshape(seq_count, CACHE_LEN, HEADS, 2, head_dim)
    scores = jnp.einsum('shmd,sjhmd->shmj', queries, cache_rows) * score_scale
    own_score = lax.optimization_barrier(jnp.sum(queries * new_keys, axis=-1)) * score_scale
    live_mask = (jnp.arange(CACHE_LEN, dtype=jnp.int32)[None, :] < seq_lengths[:, None])[:, None, None, :]
    peak_score = jnp.maximum(lax.optimization_barrier(jnp.max(jnp.where(live_mask, scores, -jnp.inf), axis=-1)), own_score)
    exp_terms = jnp.where(live_mask, jnp.exp(scores - peak_score[..., None]), 0.0)
    own_term = jnp.exp(own_score - peak_score)
    denom_sum = lax.optimization_barrier(jnp.sum(exp_terms, axis=-1)) + own_term
    map_probs = exp_terms / denom_sum[..., None]
    own_prob = own_term / denom_sum
    lambda_row = lambdas[None, :]
    mixture = rounded(map_probs[:, :, 0] - lambda_row[..., None] * map_probs[:, :, 1])
    own_mixture = rounded(own_prob[:, :, 0] - lambda_row * own_prob[:, :, 1])
    head_out = jnp.einsum('shj,sjhv->shv', mixture, past_values.astype(jnp.float32))
    return head_out + own_mixture[..., None] * new_values

def reference(tokens, attn_gain, query_weight, key_weight, value_weight, out_weight, lambdas, head_gain, cache_keys, cache_values, lengths, moe_gain, gate_weight, up_weight, down_weight, shared_gate, shared_up, shared_down, expert_ids, expert_weights):
    normed = rms_scale(tokens, attn_gain).astype(jnp.bfloat16)
    query_rows = jnp.dot(normed, query_weight, preferred_element_type=jnp.float32).astype(jnp.bfloat16)
    key_new = jnp.dot(normed, key_weight, preferred_element_type=jnp.float32).astype(jnp.bfloat16)
    value_new = jnp.dot(normed, value_weight, preferred_element_type=jnp.float32).astype(jnp.bfloat16)

    def grouped(array):
        return array.reshape((N_EP, SEQ_DEV) + array.shape[1:])
    head_out = lax.map(lambda blocks: attend_group(blocks, lambdas), (grouped(query_rows), grouped(key_new), grouped(value_new), grouped(cache_keys), grouped(cache_values), grouped(lengths)))
    head_out = head_out.reshape(SEQS, HEADS, VD)
    head_normed = rms_scale(head_out, head_gain).astype(jnp.bfloat16)
    group_cols = HEADS * VD // N_TP
    head_groups = head_normed.reshape(SEQS, N_TP, group_cols).astype(jnp.float32)
    out_groups = out_weight.reshape(D, N_TP, group_cols).astype(jnp.float32)
    attn_part = rounded(jnp.einsum('snc,dnc->nsd', head_groups, out_groups))
    mixed_rows = (tokens.astype(jnp.float32) + lax.optimization_barrier(jnp.sum(attn_part, axis=0))).astype(jnp.bfloat16)
    moe_normed = rms_scale(mixed_rows, moe_gain).astype(jnp.bfloat16)
    shared_gate_out = jnp.dot(moe_normed, shared_gate, preferred_element_type=jnp.float32)
    shared_up_out = jnp.dot(moe_normed, shared_up, preferred_element_type=jnp.float32)
    shared_hidden = (jax.nn.silu(shared_gate_out) * shared_up_out).astype(jnp.bfloat16)
    shared_cols = SW // N_TP
    shared_part = rounded(jnp.einsum('snc,ncd->nsd', shared_hidden.reshape(SEQS, N_TP, shared_cols).astype(jnp.float32), shared_down.reshape(N_TP, shared_cols, D).astype(jnp.float32)))
    shared_out = lax.optimization_barrier(jnp.sum(shared_part, axis=0))
    slot_ids = expert_ids.reshape(N_EP, SEQ_DEV * TOP).astype(jnp.int32)
    expert_hits = (slot_ids[..., None] == jnp.arange(EXPERTS, dtype=jnp.int32)[None, None, :]).astype(jnp.int32)
    earlier = jnp.cumsum(expert_hits, axis=1).astype(jnp.int32) - expert_hits
    slot_rank = lax.optimization_barrier(jnp.sum(earlier * expert_hits, axis=-1)).astype(jnp.int32)
    slot_row = (jnp.arange(N_EP, dtype=jnp.int32)[:, None] * CAP + slot_rank).reshape(-1)
    slot_token = (jnp.arange(SEQS * TOP, dtype=jnp.int32) // TOP).astype(jnp.int32)
    flat_ids = slot_ids.reshape(-1)
    expert_rows = jnp.zeros((EXPERTS, N_EP * CAP, D), jnp.bfloat16)
    expert_rows = expert_rows.at[flat_ids, slot_row].set(moe_normed[slot_token])
    expert_cols = EW // N_TP

    def run_expert(blocks):
        row_block, gate_block, up_block, down_block = blocks
        gate_out = jnp.dot(row_block, gate_block, preferred_element_type=jnp.float32)
        up_out = jnp.dot(row_block, up_block, preferred_element_type=jnp.float32)
        expert_hidden = (jax.nn.silu(gate_out) * up_out).astype(jnp.bfloat16)
        partials = jnp.einsum('rnc,ncd->nrd', expert_hidden.reshape(N_EP * CAP, N_TP, expert_cols).astype(jnp.float32), down_block.reshape(N_TP, expert_cols, D).astype(jnp.float32))
        return lax.optimization_barrier(jnp.sum(rounded(partials), axis=0)).astype(jnp.bfloat16)
    expert_out = lax.map(run_expert, (expert_rows, gate_weight, up_weight, down_weight))
    slot_values = expert_out[flat_ids, slot_row].astype(jnp.float32).reshape(SEQS, TOP, D)
    routed = lax.optimization_barrier(jnp.sum(expert_weights[:, :, None] * slot_values, axis=1))
    return (mixed_rows.astype(jnp.float32) + routed + shared_out).astype(jnp.bfloat16)
```

```python
import jax
import jax.numpy as jnp
from jax import lax
from jax.experimental import pallas as pl
from jax.experimental.pallas import tpu as pltpu
from jax.sharding import PartitionSpec as P

epsilon = 1e-06
GRAIN = 128
CHUNK = 1024
PIECES = 1
FLIGHT = 3
AHEAD = 7
OUT_AT = 1
SHARES_FLOPS = 4_000_000_000


def rms_scale(values, gain):
    wide = values.astype(jnp.float32)
    return (
        wide
        * lax.rsqrt(jnp.mean(wide * wide, axis=-1, keepdims=True) + epsilon)
        * gain.astype(jnp.float32)
    )


def attend_body(
    lengths_hbm,
    lambdas_hbm,
    tokens_hbm,
    attn_gain_hbm,
    head_gain_hbm,
    query_hbm,
    key_hbm,
    value_hbm,
    out_hbm,
    keys_hbm,
    values_hbm,
    part_out,
    lengths,
    lambdas,
    tokens,
    attn_gain,
    head_gain,
    query_w,
    key_w,
    value_w,
    out_w,
    keys,
    values,
    scores,
    peaks,
    own_scores,
    queries,
    new_keys,
    new_values,
    head_outs,
    head_rows,
    small_sems,
    weight_sems,
    key_sems,
    value_sems,
):
    seq_dev = tokens.shape[0]
    heads = queries.shape[1]
    width = queries.shape[2]
    head_dim = width // 2
    cache_rows = keys.shape[1]
    scale = head_dim ** (-0.5)
    grain_rows = GRAIN * heads
    span = query_w.shape[0] // PIECES

    def weight_copy(i, piece):
        source = (query_hbm, key_hbm, value_hbm, out_hbm)[i]
        target = (query_w, key_w, value_w, out_w)[i]
        rows = pl.ds(piece * span, span)
        return pltpu.make_async_copy(source.at[rows], target.at[rows], weight_sems.at[i, piece])

    def live_rows(s):
        return pl.multiple_of((lengths[s] + GRAIN - 1) // GRAIN * grain_rows, grain_rows)

    def key_copy(s):
        rows = pl.ds(0, live_rows(s))
        return pltpu.make_async_copy(keys_hbm.at[s, rows], keys.at[s, rows], key_sems.at[s])

    def value_copy(s):
        rows = pl.ds(0, live_rows(s))
        return pltpu.make_async_copy(values_hbm.at[s, rows], values.at[s, rows], value_sems.at[s])

    small = [
        pltpu.make_async_copy(source, target, small_sems.at[i])
        for i, (source, target) in enumerate(
            (
                (lengths_hbm, lengths),
                (lambdas_hbm, lambdas),
                (tokens_hbm, tokens),
                (attn_gain_hbm, attn_gain),
                (head_gain_hbm, head_gain),
            )
        )
    ]
    for copy in small:
        copy.start()
    queue = [(weight_copy, (i, piece)) for i in range(3) for piece in range(PIECES)]
    for s in range(AHEAD):
        queue += [(key_copy, (s,)), (value_copy, (s,))]

    def start_next():
        if queue:
            make, where = queue.pop(0)
            make(*where).start()

    for _ in range(FLIGHT):
        start_next()
    for copy in small:
        copy.wait()

    def clear_tail(s, carry):
        def clear(g, carry):
            rows = pl.ds(pl.multiple_of(g * grain_rows, grain_rows), grain_rows)
            keys[s, rows, :] = jnp.zeros((grain_rows, width), jnp.bfloat16)
            values[s, rows, :] = jnp.zeros((grain_rows, width), jnp.bfloat16)
            return carry

        used = jnp.where(lengths[s] > cache_rows // heads // 2, cache_rows, cache_rows // 2)
        return lax.fori_loop(live_rows(s) // grain_rows, used // grain_rows, clear, carry)

    lax.fori_loop(0, seq_dev, clear_tail, 0)

    normed = rms_scale(tokens[...], attn_gain[...].astype(jnp.float32).reshape(1, -1)).astype(jnp.bfloat16)
    for i, (weight, target) in enumerate(
        ((query_w, queries), (key_w, new_keys), (value_w, new_values))
    ):
        rows = None
        for piece in range(PIECES):
            weight_copy(i, piece).wait()
            start_next()
            lines = slice(piece * span, (piece + 1) * span)
            more = jnp.dot(normed[:, lines], weight[lines, :], preferred_element_type=jnp.float32)
            rows = more if rows is None else rows + more
        rows = rows.astype(jnp.bfloat16).astype(jnp.float32)
        for s in range(seq_dev):
            for h in range(heads):
                target[s, h : h + 1, :] = rows[s : s + 1, h * width : (h + 1) * width]

    while queue:
        start_next()
    lane = lax.broadcasted_iota(jnp.int32, (2 * heads, width), 1)
    row = lax.broadcasted_iota(jnp.int32, (2 * heads, width), 0)
    map_mask = (lane < head_dim) == (row < heads)
    lane_or_far = jnp.where(lane % heads == row % heads, lane, jnp.int32(1 << 30))
    head_row = lax.broadcasted_iota(jnp.int32, (heads, 1), 0)
    lam = jnp.zeros((heads, 1), jnp.float32)
    for h in range(heads):
        lam = jnp.where(head_row == h, lambdas[h], lam)

    def score_stage(s, size):
        slot = s % 2
        live = lengths[s] * heads
        query = queries[s]
        query16 = jnp.where(map_mask, jnp.concatenate([query, query], axis=0), 0.0)
        fresh = new_keys[s]
        fresh16 = jnp.concatenate([fresh, fresh], axis=0)
        own = jnp.sum(query16 * fresh16, axis=1, keepdims=True) * scale
        query16 = (query16 * scale).astype(jnp.bfloat16)
        none = jnp.zeros_like(query16)
        query32 = jnp.concatenate(
            [
                jnp.concatenate([query16, none], axis=1),
                jnp.concatenate([none, query16], axis=1),
            ],
            axis=0,
        )
        half = size * heads // 2
        peak = jnp.full((2 * heads, width), -jnp.inf, jnp.float32)
        for c in range(0, half, CHUNK):
            pair = jnp.concatenate(
                [keys[s, c : c + CHUNK, :], keys[s, half + c : half + c + CHUNK, :]], axis=1
            )
            block = lax.dot_general(
                query32, pair, (((1,), (1,)), ((), ())), preferred_element_type=jnp.float32
            )
            for part in range(2):
                for j in range(0, CHUNK, width):
                    start = part * half + c + j
                    tile = block[part * 2 * heads : (part + 1) * 2 * heads, j : j + width]
                    tile = jnp.where(lane_or_far < live - start, tile, -jnp.inf)
                    scores[slot, :, start : start + width] = tile
                    peak = jnp.maximum(peak, tile)
        peak = jnp.maximum(jnp.max(peak, axis=1, keepdims=True), own)
        peaks[slot] = jnp.broadcast_to(peak, (2 * heads, width))
        own_scores[slot] = jnp.broadcast_to(own, (2 * heads, width))

    def value_stage(s, size):
        slot = s % 2
        rows = size * heads
        half = rows // 2
        peak = peaks[slot]
        own_term = jnp.exp(own_scores[slot] - peak)
        sums = [jnp.zeros((2 * heads, width), jnp.float32) for _ in range(4)]
        for i, start in enumerate(range(0, rows, width)):
            tile = jnp.exp(scores[slot, :, start : start + width] - peak)
            scores[slot, :, start : start + width] = tile
            sums[i % 4] = sums[i % 4] + tile
        total = (sums[0] + sums[1]) + (sums[2] + sums[3])
        inverse = 1.0 / (jnp.sum(total, axis=1, keepdims=True) + own_term)
        first = inverse[:heads]
        second = lam * inverse[heads:]
        acc = jnp.zeros((2 * heads, 2 * width), jnp.float32)
        for c in range(0, half, CHUNK):
            tiles = []
            for j in range(c, c + CHUNK, width):
                mixed = [
                    scores[slot, :heads, start : start + width] * first
                    - scores[slot, heads:, start : start + width] * second
                    for start in (j, half + j)
                ]
                tiles.append(jnp.concatenate(mixed, axis=0).astype(jnp.bfloat16))
            pair = jnp.concatenate(
                [values[s, c : c + CHUNK, :], values[s, half + c : half + c + CHUNK, :]], axis=1
            )
            acc = acc + jnp.dot(
                jnp.concatenate(tiles, axis=1), pair, preferred_element_type=jnp.float32
            )
        own_mixture = own_term[:heads] * first - own_term[heads:] * second
        own_mixture = own_mixture.astype(jnp.bfloat16).astype(jnp.float32)
        head_outs[s] = acc[:heads, :width] + acc[heads:, width:] + own_mixture * new_values[s]

    full = cache_rows // heads
    sizes = (full // 2, full)

    def sized(run, s):
        for size in sizes:

            @pl.when((lengths[s] > sizes[0]) == (size == full))
            def _():
                run(s, size)

    key_copy(0).wait()
    sized(score_stage, 0)

    def stage(s, carry):
        key_copy(s).wait()
        value_copy(s - 1).wait()

        @pl.when(s + AHEAD - 1 < seq_dev)
        def _():
            key_copy(s + AHEAD - 1).start()
            value_copy(s + AHEAD - 1).start()

        @pl.when(s == OUT_AT)
        def _():
            for piece in range(PIECES):
                weight_copy(3, piece).start()

        sized(score_stage, s)
        sized(value_stage, s - 1)
        return carry

    lax.fori_loop(1, seq_dev, stage, 0)
    value_copy(seq_dev - 1).wait()
    sized(value_stage, seq_dev - 1)
    head_normed = rms_scale(head_outs[...], head_gain[...].reshape(1, 1, width))
    for s in range(seq_dev):
        for h in range(heads):
            head_rows[s : s + 1, h * width : (h + 1) * width] = head_normed[s, h : h + 1, :]
    for piece in range(PIECES):
        weight_copy(3, piece).wait()
    part = lax.dot_general(
        head_rows[:seq_dev, :].astype(jnp.bfloat16),
        out_w[...],
        (((1,), (1,)), ((), ())),
        preferred_element_type=jnp.float32,
    )
    part_out[...] = part.astype(jnp.bfloat16)


def attend_kernel(
    tokens,
    attn_gain,
    query_weight,
    key_weight,
    value_weight,
    out_weight,
    lambdas,
    head_gain,
    cache_keys,
    cache_values,
    lengths,
):
    seq_dev, model_width = tokens.shape
    _, cache_len, heads, width = cache_keys.shape
    cols = heads * width
    rows = cache_len * heads
    vmem = pl.BlockSpec(memory_space=pltpu.VMEM)
    anywhere = pl.BlockSpec(memory_space=pltpu.HBM)
    bf16, f32 = jnp.bfloat16, jnp.float32
    return pl.pallas_call(
        attend_body,
        out_shape=jax.ShapeDtypeStruct((seq_dev, model_width), bf16),
        in_specs=[anywhere] * 11,
        out_specs=vmem,
        scratch_shapes=[
            pltpu.SMEM((seq_dev,), jnp.int32),
            pltpu.SMEM((heads,), f32),
            pltpu.VMEM((seq_dev, model_width), bf16),
            pltpu.VMEM((model_width,), bf16),
            pltpu.VMEM((1, width), bf16),
            pltpu.VMEM((model_width, cols), bf16),
            pltpu.VMEM((model_width, cols), bf16),
            pltpu.VMEM((model_width, cols), bf16),
            pltpu.VMEM((model_width, cols), bf16),
            pltpu.VMEM((seq_dev, rows, width), bf16),
            pltpu.VMEM((seq_dev, rows, width), bf16),
            pltpu.VMEM((2, 2 * heads, rows), f32),
            pltpu.VMEM((2, 2 * heads, width), f32),
            pltpu.VMEM((2, 2 * heads, width), f32),
            pltpu.VMEM((seq_dev, heads, width), f32),
            pltpu.VMEM((seq_dev, heads, width), f32),
            pltpu.VMEM((seq_dev, heads, width), f32),
            pltpu.VMEM((seq_dev, heads, width), f32),
            pltpu.VMEM((seq_dev + 1, cols), f32),
            pltpu.SemaphoreType.DMA((5,)),
            pltpu.SemaphoreType.DMA((4, PIECES)),
            pltpu.SemaphoreType.DMA((seq_dev,)),
            pltpu.SemaphoreType.DMA((seq_dev,)),
        ],
        compiler_params=pltpu.CompilerParams(vmem_limit_bytes=54 << 20),
        name="attend",
    )(
        lengths,
        lambdas,
        tokens,
        attn_gain,
        head_gain.reshape(1, -1),
        query_weight,
        key_weight,
        value_weight,
        out_weight,
        cache_keys.reshape(seq_dev, rows, width),
        cache_values.reshape(seq_dev, rows, width),
    )


def slot_map(shape, cap, rows_at, slots_at):
    packed = lax.broadcasted_iota(jnp.int32, shape, rows_at)
    padded = lax.broadcasted_iota(jnp.int32, shape, slots_at)
    rank = jnp.full(shape, -7, jnp.int32)
    place = jnp.full(shape, -9, jnp.int32)
    for c in range(shape[slots_at] // 8):
        inside = (packed >= c * cap) & (packed < (c + 1) * cap)
        inside = inside & (padded >= c * 8) & (padded < (c + 1) * 8)
        rank = jnp.where(inside, packed - c * cap, rank)
        place = jnp.where(inside, padded - c * 8, place)
    return rank.astype(jnp.float32), place.astype(jnp.float32)


def slot_codes(ids, experts):
    seq_dev, top_count = ids.shape
    expert = lax.broadcasted_iota(jnp.int32, (seq_dev, experts), 1)
    hits = jnp.zeros((seq_dev, experts), jnp.float32)
    for k in range(top_count):
        hits = hits + jnp.where(ids[:, k : k + 1] == expert, 1.0, 0.0)
    earlier = lax.broadcasted_iota(jnp.int32, (seq_dev, seq_dev), 0)
    earlier = earlier > lax.broadcasted_iota(jnp.int32, (seq_dev, seq_dev), 1)
    rank = jnp.dot(
        jnp.where(earlier, 1.0, 0.0).astype(jnp.bfloat16),
        hits.astype(jnp.bfloat16),
        preferred_element_type=jnp.float32,
    )
    return jnp.where(hits > 0.5, rank, -1.0)


def padded_rows(rows, value):
    seq_dev, cols = rows.shape
    if seq_dev == 8:
        return rows
    return jnp.concatenate([rows, jnp.full((8 - seq_dev, cols), value, rows.dtype)], axis=0)


def prepare_body(index, tokens, own_part, other_part, gain, ids, mixed_out, normed_out, send_out):
    experts, block, lanes = send_out.shape
    cols = tokens.shape[1] // 2
    chunks = cols // lanes
    cap = capacity_of(tokens.shape[0], ids.shape[1], experts)
    total = own_part[...].astype(jnp.float32) + other_part[...].astype(jnp.float32)
    mixed = (tokens[...].astype(jnp.float32) + total).astype(jnp.bfloat16)
    mixed_out[...] = mixed
    normed = rms_scale(mixed, gain[...]).astype(jnp.bfloat16)
    normed_out[...] = normed
    codes = padded_rows(slot_codes(ids[...], experts), -1.0)
    codes = jnp.concatenate([codes] * chunks, axis=0)
    expert = lax.broadcasted_iota(jnp.int32, (experts, experts), 0)
    eye = expert == lax.broadcasted_iota(jnp.int32, (experts, experts), 1)
    code_rows = lax.dot_general(
        jnp.where(eye, 1.0, 0.0).astype(jnp.bfloat16),
        codes.astype(jnp.bfloat16),
        (((1,), (1,)), ((), ())),
        preferred_element_type=jnp.float32,
    )
    rank, _ = slot_map((block, chunks * 8), cap, 0, 1)
    picks = [jnp.where(code_rows[e : e + 1, :] == rank, 1.0, 0.0) for e in range(experts)]
    picks = jnp.concatenate(picks, axis=0).astype(jnp.bfloat16)
    wide = padded_rows(normed.astype(jnp.float32), 0.0)
    low = index[0] == 0
    stack = [
        jnp.where(
            low, wide[:, c * lanes : (c + 1) * lanes], wide[:, cols + c * lanes : cols + (c + 1) * lanes]
        )
        for c in range(chunks)
    ]
    stack = jnp.concatenate(stack, axis=0).astype(jnp.bfloat16)
    send = jnp.dot(picks, stack, preferred_element_type=jnp.float32).astype(jnp.bfloat16)
    for e in range(experts):
        send_out[e] = send[e * block : (e + 1) * block]


def shares_body(ids, weights, after, high_out, low_out):
    experts, padded, block = high_out.shape
    chunks = padded // 8
    seq_dev, top_count = ids.shape
    cap = capacity_of(seq_dev, top_count, experts)
    codes = padded_rows(slot_codes(ids[...], experts), -1.0)
    expert = lax.broadcasted_iota(jnp.int32, (seq_dev, experts), 1)
    shares = jnp.zeros((seq_dev, experts), jnp.float32)
    for k in range(top_count):
        shares = shares + jnp.where(ids[:, k : k + 1] == expert, weights[:, k : k + 1], 0.0)
    codes = jnp.concatenate([codes] * chunks, axis=0)
    shares = jnp.concatenate([padded_rows(shares, 0.0)] * chunks, axis=0)
    rank, _ = slot_map((padded, block), cap, 1, 0)
    for e in range(experts):
        share = jnp.where(codes[:, e : e + 1] == rank, shares[:, e : e + 1], 0.0)
        high = share.astype(jnp.bfloat16)
        high_out[e] = high
        low_out[e] = (share - high.astype(jnp.float32)).astype(jnp.bfloat16)


def expert_body(
    index, own, other, gate_hbm, up_hbm, down_hbm, own_out, sent_out, rows, gate, up, down, sems
):
    pairs = ((gate_hbm, gate), (up_hbm, up), (down_hbm, down))
    copies = [pltpu.make_async_copy(a, b, sems.at[i]) for i, (a, b) in enumerate(pairs)]
    for copy in copies:
        copy.start()
    experts, block, lanes = own.shape
    cols = rows.shape[1] // 2
    chunks = cols // lanes
    cap = block_cap(block, chunks)
    tp = index[0]
    rank, place = slot_map((chunks * 8, block), cap, 1, 0)
    spread = jnp.where(rank == place, 1.0, 0.0).astype(jnp.bfloat16)
    rank, place = slot_map((block, chunks * 8), cap, 0, 1)
    gather = jnp.where(rank == place, 1.0, 0.0).astype(jnp.bfloat16)
    for source, half in ((own, tp), (other, 1 - tp)):
        start = half * cols
        for e in range(experts):
            got = jnp.dot(spread, source[e], preferred_element_type=jnp.float32)
            for c in range(chunks):
                at = pl.ds(pl.multiple_of(start + c * lanes, lanes), lanes)
                rows[e * 8 : (e + 1) * 8, at] = got[c * 8 : (c + 1) * 8]
    x = rows[...].astype(jnp.bfloat16)
    copies[0].wait()
    gate_part = jnp.dot(x, gate[...], preferred_element_type=jnp.float32)
    copies[1].wait()
    up_part = jnp.dot(x, up[...], preferred_element_type=jnp.float32)
    hidden = (gate_part / (1.0 + jnp.exp(-gate_part)) * up_part).astype(jnp.bfloat16)
    copies[2].wait()
    rows[...] = jnp.dot(hidden, down[...], preferred_element_type=jnp.float32)
    for target, half in ((sent_out, 1 - tp), (own_out, tp)):
        start = half * cols
        for e in range(experts):
            tiles = [
                rows[e * 8 : (e + 1) * 8, pl.ds(pl.multiple_of(start + c * lanes, lanes), lanes)]
                for c in range(chunks)
            ]
            tiles = jnp.concatenate(tiles, axis=0).astype(jnp.bfloat16)
            packed = jnp.dot(gather, tiles, preferred_element_type=jnp.float32)
            target[e] = packed.astype(jnp.bfloat16)


def combine_body(index, returned, high, low, mixed, own_shared, other_shared, result):
    experts, block, lanes = returned.shape
    cols = result.shape[1]
    seq_dev = result.shape[0]
    acc = jnp.zeros((high.shape[1], lanes), jnp.float32)
    for e in range(experts):
        acc = acc + jnp.dot(high[e], returned[e], preferred_element_type=jnp.float32)
        acc = acc + jnp.dot(low[e], returned[e], preferred_element_type=jnp.float32)
    first = index[0] == 0
    for c in range(cols // lanes):
        left = slice(c * lanes, (c + 1) * lanes)
        right = slice(cols + c * lanes, cols + (c + 1) * lanes)
        kept = jnp.where(first, mixed[:, left].astype(jnp.float32), mixed[:, right].astype(jnp.float32))
        own = jnp.where(
            first, own_shared[:, left].astype(jnp.float32), own_shared[:, right].astype(jnp.float32)
        )
        shared = own + other_shared[:, left].astype(jnp.float32)
        total = kept + acc[c * 8 : c * 8 + seq_dev] + shared
        result[:, left] = total.astype(jnp.bfloat16)


def capacity_of(seq_dev, top_count, experts):
    return min(seq_dev, max(2, 2 * seq_dev * top_count // experts))


def block_cap(block, chunks):
    return block // chunks


def routed_pair(
    tokens,
    attn_part,
    moe_gain,
    gate_weight,
    up_weight,
    down_weight,
    shared_gate,
    shared_up,
    shared_down,
    expert_ids,
    expert_weights,
):
    seq_dev, model_width = tokens.shape
    experts = lax.axis_size("ep")
    cols = model_width // 2
    lanes = 128
    chunks = cols // lanes
    cap = capacity_of(seq_dev, expert_ids.shape[1], experts)
    block = (cap * chunks + 15) // 16 * 16
    bf16 = jnp.bfloat16
    vmem = pl.BlockSpec(memory_space=pltpu.VMEM)
    smem = pl.BlockSpec(memory_space=pltpu.SMEM)
    anywhere = pl.BlockSpec(memory_space=pltpu.HBM)
    swap = [(0, 1), (1, 0)]
    index = lax.axis_index("tp").astype(jnp.int32).reshape(1)
    other_part = lax.ppermute(attn_part, "tp", swap)
    shape = jax.ShapeDtypeStruct
    packed = shape((experts, block, lanes), bf16)
    rows = shape((seq_dev, model_width), bf16)
    mixed, normed, send = pl.pallas_call(
        prepare_body,
        out_shape=(rows, rows, packed),
        in_specs=[smem] + [vmem] * 5,
        out_specs=(vmem,) * 3,
        compiler_params=pltpu.CompilerParams(vmem_limit_bytes=8 << 20),
        name="prepare",
    )(index, tokens, attn_part, other_part, moe_gain.reshape(1, -1), expert_ids)
    arrived = lax.all_to_all(send, "ep", split_axis=0, concat_axis=0, tiled=True)
    hidden = gate_weight.shape[2]
    mix = shape((experts, chunks * 8, block), bf16)
    high, low = pl.pallas_call(
        shares_body,
        out_shape=(mix, mix),
        in_specs=[vmem, vmem, anywhere],
        out_specs=(vmem,) * 2,
        compiler_params=pltpu.CompilerParams(vmem_limit_bytes=8 << 20),
        cost_estimate=pl.CostEstimate(
            flops=SHARES_FLOPS, transcendentals=0, bytes_accessed=4 * experts * chunks * 8 * block
        ),
        name="shares",
    )(expert_ids, expert_weights, normed)
    arrived, high = lax.optimization_barrier((arrived, high))
    partner = lax.ppermute(arrived, "tp", swap)
    own_out, sent_out = pl.pallas_call(
        expert_body,
        out_shape=(packed, packed),
        in_specs=[smem] + [vmem] * 2 + [anywhere] * 3,
        out_specs=(vmem,) * 2,
        scratch_shapes=[
            pltpu.VMEM((experts * 8, model_width), jnp.float32),
            pltpu.VMEM((model_width, hidden), bf16),
            pltpu.VMEM((model_width, hidden), bf16),
            pltpu.VMEM((hidden, model_width), bf16),
            pltpu.SemaphoreType.DMA((3,)),
        ],
        compiler_params=pltpu.CompilerParams(vmem_limit_bytes=24 << 20),
        name="expert",
    )(
        index,
        arrived,
        partner,
        *(
            pltpu.with_memory_space_constraint(weight[0], pltpu.HBM)
            for weight in (gate_weight, up_weight, down_weight)
        ),
    )
    expert_sum = own_out.astype(jnp.float32) + lax.ppermute(sent_out, "tp", swap).astype(jnp.float32)
    returned = lax.all_to_all(
        expert_sum.astype(bf16), "ep", split_axis=0, concat_axis=0, tiled=True
    )
    shared_gate_out = jnp.dot(normed, shared_gate, preferred_element_type=jnp.float32)
    shared_up_out = jnp.dot(normed, shared_up, preferred_element_type=jnp.float32)
    shared_hidden = (jax.nn.silu(shared_gate_out) * shared_up_out).astype(bf16)
    shared_part = jnp.dot(shared_hidden, shared_down, preferred_element_type=jnp.float32)
    shared_part = shared_part.astype(bf16)
    shared_sent = lax.dynamic_slice_in_dim(shared_part, (1 - index[0]) * cols, cols, 1)
    shared_other = lax.ppermute(shared_sent, "tp", swap)
    return pl.pallas_call(
        combine_body,
        out_shape=shape((seq_dev, cols), bf16),
        in_specs=[smem] + [vmem] * 6,
        out_specs=vmem,
        compiler_params=pltpu.CompilerParams(vmem_limit_bytes=8 << 20),
        name="combine",
    )(index, returned, high, low, mixed, shared_part, shared_other)


def attend_plain(
    tokens,
    attn_gain,
    query_weight,
    key_weight,
    value_weight,
    out_weight,
    lambdas,
    head_gain,
    cache_keys,
    cache_values,
    lengths,
):
    seq_dev, model_width = tokens.shape
    local_heads = lambdas.shape[0]
    head_dim = cache_keys.shape[-1] // 2
    cache_len = cache_keys.shape[1]
    normed = rms_scale(tokens, attn_gain).astype(jnp.bfloat16)
    query_rows = jnp.dot(normed, query_weight, preferred_element_type=jnp.float32).astype(
        jnp.bfloat16
    )
    key_new = jnp.dot(normed, key_weight, preferred_element_type=jnp.float32).astype(jnp.bfloat16)
    value_new = jnp.dot(normed, value_weight, preferred_element_type=jnp.float32).astype(
        jnp.bfloat16
    )
    score_scale = head_dim ** (-0.5)
    queries = query_rows.reshape(seq_dev, local_heads, 2, head_dim)
    new_keys = key_new.reshape(seq_dev, local_heads, 2, head_dim)
    new_values = value_new.reshape(seq_dev, local_heads, 2 * head_dim)
    past_keys = cache_keys.reshape(seq_dev, cache_len, local_heads, 2, head_dim)
    scores = (
        jnp.einsum("shmd,sjhmd->shmj", queries, past_keys, preferred_element_type=jnp.float32)
        * score_scale
    )
    own_score = (
        jnp.sum(queries.astype(jnp.float32) * new_keys.astype(jnp.float32), axis=-1) * score_scale
    )
    live_mask = (jnp.arange(cache_len, dtype=jnp.int32)[None, :] < lengths[:, None])[
        :, None, None, :
    ]
    peak_score = jnp.maximum(jnp.max(jnp.where(live_mask, scores, -jnp.inf), axis=-1), own_score)
    exp_terms = jnp.where(live_mask, jnp.exp(scores - peak_score[..., None]), 0.0)
    own_term = jnp.exp(own_score - peak_score)
    denom_sum = jnp.sum(exp_terms, axis=-1) + own_term
    map_probs = exp_terms / denom_sum[..., None]
    own_prob = own_term / denom_sum
    lambda_row = lambdas[None, :]
    mixture = (map_probs[:, :, 0] - lambda_row[..., None] * map_probs[:, :, 1]).astype(jnp.bfloat16)
    own_mixture = (own_prob[:, :, 0] - lambda_row * own_prob[:, :, 1]).astype(jnp.bfloat16)
    head_out = jnp.einsum(
        "shj,sjhv->shv", mixture, cache_values, preferred_element_type=jnp.float32
    )
    head_out = head_out + own_mixture.astype(jnp.float32)[..., None] * new_values.astype(
        jnp.float32
    )
    head_normed = (
        rms_scale(head_out, head_gain)
        .astype(jnp.bfloat16)
        .reshape(seq_dev, local_heads * 2 * head_dim)
    )
    return lax.dot_general(
        head_normed, out_weight, (((1,), (1,)), ((), ())), preferred_element_type=jnp.float32
    ).astype(jnp.bfloat16)


def scatter_sum(part):
    part = part.astype(jnp.bfloat16)
    if lax.axis_size("tp") != 2:
        return lax.psum_scatter(part, "tp", scatter_dimension=1, tiled=True).astype(jnp.float32)
    cols = part.shape[1] // 2
    index = lax.axis_index("tp")
    own = lax.dynamic_slice_in_dim(part, index * cols, cols, 1)
    sent = lax.dynamic_slice_in_dim(part, (1 - index) * cols, cols, 1)
    arrived = lax.ppermute(sent, "tp", [(0, 1), (1, 0)])
    return own.astype(jnp.float32) + arrived.astype(jnp.float32)


def shards(
    tokens,
    attn_gain,
    query_weight,
    key_weight,
    value_weight,
    out_weight,
    lambdas,
    head_gain,
    cache_keys,
    cache_values,
    lengths,
    moe_gain,
    gate_weight,
    up_weight,
    down_weight,
    shared_gate,
    shared_up,
    shared_down,
    expert_ids,
    expert_weights,
):
    seq_dev, model_width = tokens.shape
    pair = lax.axis_size("tp") == 2 and model_width % 256 == 0 and seq_dev <= 8
    attend = attend_kernel if pair else attend_plain
    attn_part = attend(
        tokens,
        attn_gain,
        query_weight,
        key_weight,
        value_weight,
        out_weight,
        lambdas,
        head_gain,
        cache_keys,
        cache_values,
        lengths,
    )
    if pair:
        return routed_pair(
            tokens,
            attn_part,
            moe_gain,
            gate_weight,
            up_weight,
            down_weight,
            shared_gate,
            shared_up,
            shared_down,
            expert_ids,
            expert_weights,
        )
    attn_total = lax.psum(attn_part, "tp").astype(jnp.float32)
    mixed_rows = (tokens.astype(jnp.float32) + attn_total).astype(jnp.bfloat16)
    moe_normed = rms_scale(mixed_rows, moe_gain).astype(jnp.bfloat16)
    shared_gate_out = jnp.dot(moe_normed, shared_gate, preferred_element_type=jnp.float32)
    shared_up_out = jnp.dot(moe_normed, shared_up, preferred_element_type=jnp.float32)
    shared_hidden = (jax.nn.silu(shared_gate_out) * shared_up_out).astype(jnp.bfloat16)
    shared_part = jnp.dot(shared_hidden, shared_down, preferred_element_type=jnp.float32)
    experts = lax.axis_size("ep")
    top_count = expert_ids.shape[1]
    capacity = min(seq_dev, max(2, 2 * seq_dev * top_count // experts))
    slot_count = seq_dev * top_count
    slot_ids = expert_ids.reshape(slot_count)
    expert_hits = (slot_ids[:, None] == jnp.arange(experts, dtype=jnp.int32)[None, :]).astype(
        jnp.int32
    )
    slot_rank = jnp.sum((jnp.cumsum(expert_hits, axis=0) - expert_hits) * expert_hits, axis=1)
    slot_place = slot_ids * capacity + slot_rank
    placed = (
        slot_place[:, None] == jnp.arange(experts * capacity, dtype=jnp.int32)[None, :]
    ).astype(jnp.bfloat16)
    slot_token = jnp.arange(slot_count, dtype=jnp.int32) // top_count
    token_pick = (slot_token[:, None] == jnp.arange(seq_dev, dtype=jnp.int32)[None, :]).astype(
        jnp.bfloat16
    )
    dispatch = lax.dot_general(
        placed, token_pick, (((0,), (0,)), ((), ())), preferred_element_type=jnp.float32
    ).astype(jnp.bfloat16)
    col_count = model_width // lax.axis_size("tp")
    own_start = lax.axis_index("tp") * col_count
    own_normed = lax.dynamic_slice_in_dim(moe_normed, own_start, col_count, 1)
    send_slice = jnp.dot(dispatch, own_normed, preferred_element_type=jnp.float32).astype(
        jnp.bfloat16
    )
    arrived = lax.all_to_all(send_slice, "ep", split_axis=0, concat_axis=0, tiled=True)
    received = lax.all_gather(arrived, "tp", axis=1, tiled=True)
    gate_out = jnp.dot(received, gate_weight[0], preferred_element_type=jnp.float32)
    up_out = jnp.dot(received, up_weight[0], preferred_element_type=jnp.float32)
    expert_hidden = (jax.nn.silu(gate_out) * up_out).astype(jnp.bfloat16)
    expert_part = jnp.dot(expert_hidden, down_weight[0], preferred_element_type=jnp.float32)
    expert_sum, shared_out = scatter_sum(expert_part), scatter_sum(shared_part)
    returned = lax.all_to_all(
        expert_sum.astype(jnp.bfloat16), "ep", split_axis=0, concat_axis=0, tiled=True
    )
    slot_values = jnp.dot(placed, returned, preferred_element_type=jnp.float32).reshape(
        seq_dev, top_count, col_count
    )
    routed = jnp.sum(expert_weights[:, :, None] * slot_values, axis=1)
    own_cols = lax.dynamic_slice_in_dim(mixed_rows, own_start, col_count, 1)
    return (own_cols.astype(jnp.float32) + routed + shared_out).astype(jnp.bfloat16)


def solution(mesh):
    in_specs = (
        P("ep", None),
        P(),
        P(None, "tp"),
        P(None, "tp"),
        P(None, "tp"),
        P(None, "tp"),
        P("tp"),
        P(),
        P("ep", None, "tp", None),
        P("ep", None, "tp", None),
        P("ep"),
        P(),
        P("ep", None, "tp"),
        P("ep", None, "tp"),
        P("ep", "tp", None),
        P(None, "tp"),
        P(None, "tp"),
        P("tp", None),
        P("ep", None),
        P("ep", None),
    )
    out_specs = P("ep", "tp")
    return jax.shard_map(shards, mesh=mesh, in_specs=in_specs, out_specs=out_specs, check_vma=False)
```

```python
import jax
import jax.numpy as jnp
from jax import lax
from jax.experimental import pallas as pl
from jax.experimental.pallas import tpu as pltpu
from jax.sharding import PartitionSpec as P

epsilon = 1e-06
GRAIN = 128
STEP = 256
CHUNK = 1024
PIECES = 1
FLIGHT = 3
AHEAD = 7
OUT_AT = 1
SHARES_FLOPS = 4_000_000_000


def rms_scale(values, gain):
    wide = values.astype(jnp.float32)
    return (
        wide
        * lax.rsqrt(jnp.mean(wide * wide, axis=-1, keepdims=True) + epsilon)
        * gain.astype(jnp.float32)
    )


def attend_body(
    lengths_hbm,
    lambdas_hbm,
    tokens_hbm,
    attn_gain_hbm,
    head_gain_hbm,
    query_hbm,
    key_hbm,
    value_hbm,
    out_hbm,
    keys_hbm,
    values_hbm,
    part_out,
    lengths,
    lambdas,
    tokens,
    attn_gain,
    head_gain,
    query_w,
    key_w,
    value_w,
    out_w,
    keys,
    values,
    scores,
    peaks,
    own_scores,
    queries,
    new_keys,
    new_values,
    head_outs,
    head_rows,
    small_sems,
    weight_sems,
    key_sems,
    value_sems,
):
    seq_dev = tokens.shape[0]
    heads = queries.shape[1]
    width = queries.shape[2]
    head_dim = width // 2
    cache_rows = keys.shape[1]
    scale = head_dim ** (-0.5)
    grain_rows = GRAIN * heads
    span = query_w.shape[0] // PIECES

    def weight_copy(i, piece):
        source = (query_hbm, key_hbm, value_hbm, out_hbm)[i]
        target = (query_w, key_w, value_w, out_w)[i]
        rows = pl.ds(piece * span, span)
        return pltpu.make_async_copy(source.at[rows], target.at[rows], weight_sems.at[i, piece])

    def live_rows(s):
        return pl.multiple_of((lengths[s] + GRAIN - 1) // GRAIN * grain_rows, grain_rows)

    def key_copy(s):
        rows = pl.ds(0, live_rows(s))
        return pltpu.make_async_copy(keys_hbm.at[s, rows], keys.at[s, rows], key_sems.at[s])

    def value_copy(s):
        rows = pl.ds(0, live_rows(s))
        return pltpu.make_async_copy(values_hbm.at[s, rows], values.at[s, rows], value_sems.at[s])

    small = [
        pltpu.make_async_copy(source, target, small_sems.at[i])
        for i, (source, target) in enumerate(
            (
                (lengths_hbm, lengths),
                (lambdas_hbm, lambdas),
                (tokens_hbm, tokens),
                (attn_gain_hbm, attn_gain),
                (head_gain_hbm, head_gain),
            )
        )
    ]
    for copy in small:
        copy.start()
    queue = [(weight_copy, (i, piece)) for i in range(3) for piece in range(PIECES)]
    for s in range(AHEAD):
        queue += [(key_copy, (s,)), (value_copy, (s,))]

    def start_next():
        if queue:
            make, where = queue.pop(0)
            make(*where).start()

    for _ in range(FLIGHT):
        start_next()
    for copy in small:
        copy.wait()

    def clear_tail(s, carry):
        def clear(g, carry):
            rows = pl.ds(pl.multiple_of(g * grain_rows, grain_rows), grain_rows)
            keys[s, rows, :] = jnp.zeros((grain_rows, width), jnp.bfloat16)
            values[s, rows, :] = jnp.zeros((grain_rows, width), jnp.bfloat16)
            return carry

        used = (lengths[s] + STEP - 1) // STEP * STEP * heads
        return lax.fori_loop(live_rows(s) // grain_rows, used // grain_rows, clear, carry)

    lax.fori_loop(0, seq_dev, clear_tail, 0)

    normed = rms_scale(tokens[...], attn_gain[...].astype(jnp.float32).reshape(1, -1)).astype(jnp.bfloat16)
    for i, (weight, target) in enumerate(
        ((query_w, queries), (key_w, new_keys), (value_w, new_values))
    ):
        rows = None
        for piece in range(PIECES):
            weight_copy(i, piece).wait()
            start_next()
            lines = slice(piece * span, (piece + 1) * span)
            more = jnp.dot(normed[:, lines], weight[lines, :], preferred_element_type=jnp.float32)
            rows = more if rows is None else rows + more
        rows = rows.astype(jnp.bfloat16).astype(jnp.float32)
        for s in range(seq_dev):
            for h in range(heads):
                target[s, h : h + 1, :] = rows[s : s + 1, h * width : (h + 1) * width]

    while queue:
        start_next()
    lane = lax.broadcasted_iota(jnp.int32, (2 * heads, width), 1)
    row = lax.broadcasted_iota(jnp.int32, (2 * heads, width), 0)
    map_mask = (lane < head_dim) == (row < heads)
    lane_or_far = jnp.where(lane % heads == row % heads, lane, jnp.int32(1 << 30))
    head_row = lax.broadcasted_iota(jnp.int32, (heads, 1), 0)
    lam = jnp.zeros((heads, 1), jnp.float32)
    for h in range(heads):
        lam = jnp.where(head_row == h, lambdas[h], lam)

    def score_stage(s, size):
        slot = s % 2
        live = lengths[s] * heads
        query = queries[s]
        query16 = jnp.where(map_mask, jnp.concatenate([query, query], axis=0), 0.0)
        fresh = new_keys[s]
        fresh16 = jnp.concatenate([fresh, fresh], axis=0)
        own = jnp.sum(query16 * fresh16, axis=1, keepdims=True) * scale
        query16 = (query16 * scale).astype(jnp.bfloat16)
        none = jnp.zeros_like(query16)
        query32 = jnp.concatenate(
            [
                jnp.concatenate([query16, none], axis=1),
                jnp.concatenate([none, query16], axis=1),
            ],
            axis=0,
        )
        half = size * heads // 2
        peak = jnp.full((2 * heads, width), -jnp.inf, jnp.float32)
        for c in range(0, half, CHUNK):
            pair = jnp.concatenate(
                [keys[s, c : c + CHUNK, :], keys[s, half + c : half + c + CHUNK, :]], axis=1
            )
            block = lax.dot_general(
                query32, pair, (((1,), (1,)), ((), ())), preferred_element_type=jnp.float32
            )
            for part in range(2):
                for j in range(0, CHUNK, width):
                    start = part * half + c + j
                    tile = block[part * 2 * heads : (part + 1) * 2 * heads, j : j + width]
                    tile = jnp.where(lane_or_far < live - start, tile, -jnp.inf)
                    scores[slot, :, start : start + width] = tile
                    peak = jnp.maximum(peak, tile)
        peak = jnp.maximum(jnp.max(peak, axis=1, keepdims=True), own)
        peaks[slot] = jnp.broadcast_to(peak, (2 * heads, width))
        own_scores[slot] = jnp.broadcast_to(own, (2 * heads, width))

    def value_stage(s, size):
        slot = s % 2
        rows = size * heads
        half = rows // 2
        peak = peaks[slot]
        own_term = jnp.exp(own_scores[slot] - peak)
        sums = [jnp.zeros((2 * heads, width), jnp.float32) for _ in range(4)]
        for i, start in enumerate(range(0, rows, width)):
            tile = jnp.exp(scores[slot, :, start : start + width] - peak)
            scores[slot, :, start : start + width] = tile
            sums[i % 4] = sums[i % 4] + tile
        total = (sums[0] + sums[1]) + (sums[2] + sums[3])
        inverse = 1.0 / (jnp.sum(total, axis=1, keepdims=True) + own_term)
        first = inverse[:heads]
        second = lam * inverse[heads:]
        acc = jnp.zeros((2 * heads, 2 * width), jnp.float32)
        for c in range(0, half, CHUNK):
            tiles = []
            for j in range(c, c + CHUNK, width):
                mixed = [
                    scores[slot, :heads, start : start + width] * first
                    - scores[slot, heads:, start : start + width] * second
                    for start in (j, half + j)
                ]
                tiles.append(jnp.concatenate(mixed, axis=0).astype(jnp.bfloat16))
            pair = jnp.concatenate(
                [values[s, c : c + CHUNK, :], values[s, half + c : half + c + CHUNK, :]], axis=1
            )
            acc = acc + jnp.dot(
                jnp.concatenate(tiles, axis=1), pair, preferred_element_type=jnp.float32
            )
        own_mixture = own_term[:heads] * first - own_term[heads:] * second
        own_mixture = own_mixture.astype(jnp.bfloat16).astype(jnp.float32)
        head_outs[s] = acc[:heads, :width] + acc[heads:, width:] + own_mixture * new_values[s]

    full = cache_rows // heads
    sizes = tuple(range(STEP, full + 1, STEP))

    def sized(run, s):
        for size in sizes:

            @pl.when((lengths[s] > size - STEP) & (lengths[s] <= size))
            def _():
                run(s, size)

    key_copy(0).wait()
    sized(score_stage, 0)

    def stage(s, carry):
        key_copy(s).wait()
        value_copy(s - 1).wait()

        @pl.when(s + AHEAD - 1 < seq_dev)
        def _():
            key_copy(s + AHEAD - 1).start()
            value_copy(s + AHEAD - 1).start()

        @pl.when(s == OUT_AT)
        def _():
            for piece in range(PIECES):
                weight_copy(3, piece).start()

        sized(score_stage, s)
        sized(value_stage, s - 1)
        return carry

    lax.fori_loop(1, seq_dev, stage, 0)
    value_copy(seq_dev - 1).wait()
    sized(value_stage, seq_dev - 1)
    head_normed = rms_scale(head_outs[...], head_gain[...].reshape(1, 1, width))
    for s in range(seq_dev):
        for h in range(heads):
            head_rows[s : s + 1, h * width : (h + 1) * width] = head_normed[s, h : h + 1, :]
    for piece in range(PIECES):
        weight_copy(3, piece).wait()
    part = lax.dot_general(
        head_rows[:seq_dev, :].astype(jnp.bfloat16),
        out_w[...],
        (((1,), (1,)), ((), ())),
        preferred_element_type=jnp.float32,
    )
    part_out[...] = part.astype(jnp.bfloat16)


def attend_kernel(
    tokens,
    attn_gain,
    query_weight,
    key_weight,
    value_weight,
    out_weight,
    lambdas,
    head_gain,
    cache_keys,
    cache_values,
    lengths,
):
    seq_dev, model_width = tokens.shape
    _, cache_len, heads, width = cache_keys.shape
    cols = heads * width
    rows = cache_len * heads
    vmem = pl.BlockSpec(memory_space=pltpu.VMEM)
    anywhere = pl.BlockSpec(memory_space=pltpu.HBM)
    bf16, f32 = jnp.bfloat16, jnp.float32
    return pl.pallas_call(
        attend_body,
        out_shape=jax.ShapeDtypeStruct((seq_dev, model_width), bf16),
        in_specs=[anywhere] * 11,
        out_specs=vmem,
        scratch_shapes=[
            pltpu.SMEM((seq_dev,), jnp.int32),
            pltpu.SMEM((heads,), f32),
            pltpu.VMEM((seq_dev, model_width), bf16),
            pltpu.VMEM((model_width,), bf16),
            pltpu.VMEM((1, width), bf16),
            pltpu.VMEM((model_width, cols), bf16),
            pltpu.VMEM((model_width, cols), bf16),
            pltpu.VMEM((model_width, cols), bf16),
            pltpu.VMEM((model_width, cols), bf16),
            pltpu.VMEM((seq_dev, rows, width), bf16),
            pltpu.VMEM((seq_dev, rows, width), bf16),
            pltpu.VMEM((2, 2 * heads, rows), f32),
            pltpu.VMEM((2, 2 * heads, width), f32),
            pltpu.VMEM((2, 2 * heads, width), f32),
            pltpu.VMEM((seq_dev, heads, width), f32),
            pltpu.VMEM((seq_dev, heads, width), f32),
            pltpu.VMEM((seq_dev, heads, width), f32),
            pltpu.VMEM((seq_dev, heads, width), f32),
            pltpu.VMEM((seq_dev + 1, cols), f32),
            pltpu.SemaphoreType.DMA((5,)),
            pltpu.SemaphoreType.DMA((4, PIECES)),
            pltpu.SemaphoreType.DMA((seq_dev,)),
            pltpu.SemaphoreType.DMA((seq_dev,)),
        ],
        compiler_params=pltpu.CompilerParams(vmem_limit_bytes=54 << 20),
        name="attend",
    )(
        lengths,
        lambdas,
        tokens,
        attn_gain,
        head_gain.reshape(1, -1),
        query_weight,
        key_weight,
        value_weight,
        out_weight,
        cache_keys.reshape(seq_dev, rows, width),
        cache_values.reshape(seq_dev, rows, width),
    )


def slot_map(shape, cap, rows_at, slots_at):
    packed = lax.broadcasted_iota(jnp.int32, shape, rows_at)
    padded = lax.broadcasted_iota(jnp.int32, shape, slots_at)
    rank = jnp.full(shape, -7, jnp.int32)
    place = jnp.full(shape, -9, jnp.int32)
    for c in range(shape[slots_at] // 8):
        inside = (packed >= c * cap) & (packed < (c + 1) * cap)
        inside = inside & (padded >= c * 8) & (padded < (c + 1) * 8)
        rank = jnp.where(inside, packed - c * cap, rank)
        place = jnp.where(inside, padded - c * 8, place)
    return rank.astype(jnp.float32), place.astype(jnp.float32)


def slot_codes(ids, experts):
    seq_dev, top_count = ids.shape
    expert = lax.broadcasted_iota(jnp.int32, (seq_dev, experts), 1)
    hits = jnp.zeros((seq_dev, experts), jnp.float32)
    for k in range(top_count):
        hits = hits + jnp.where(ids[:, k : k + 1] == expert, 1.0, 0.0)
    earlier = lax.broadcasted_iota(jnp.int32, (seq_dev, seq_dev), 0)
    earlier = earlier > lax.broadcasted_iota(jnp.int32, (seq_dev, seq_dev), 1)
    rank = jnp.dot(
        jnp.where(earlier, 1.0, 0.0).astype(jnp.bfloat16),
        hits.astype(jnp.bfloat16),
        preferred_element_type=jnp.float32,
    )
    return jnp.where(hits > 0.5, rank, -1.0)


def padded_rows(rows, value):
    seq_dev, cols = rows.shape
    if seq_dev == 8:
        return rows
    return jnp.concatenate([rows, jnp.full((8 - seq_dev, cols), value, rows.dtype)], axis=0)


def prepare_body(
    index, tokens, own_hbm, other_part, gain, ids, mixed_out, normed_out, send_out, own_part, sem
):
    copy = pltpu.make_async_copy(own_hbm, own_part, sem)
    copy.start()
    experts, block, lanes = send_out.shape
    cols = tokens.shape[1] // 2
    chunks = cols // lanes
    cap = capacity_of(tokens.shape[0], ids.shape[1], experts)
    codes = padded_rows(slot_codes(ids[...], experts), -1.0)
    codes = jnp.concatenate([codes] * chunks, axis=0)
    expert = lax.broadcasted_iota(jnp.int32, (experts, experts), 0)
    eye = expert == lax.broadcasted_iota(jnp.int32, (experts, experts), 1)
    code_rows = lax.dot_general(
        jnp.where(eye, 1.0, 0.0).astype(jnp.bfloat16),
        codes.astype(jnp.bfloat16),
        (((1,), (1,)), ((), ())),
        preferred_element_type=jnp.float32,
    )
    rank, _ = slot_map((block, chunks * 8), cap, 0, 1)
    picks = [jnp.where(code_rows[e : e + 1, :] == rank, 1.0, 0.0) for e in range(experts)]
    picks = jnp.concatenate(picks, axis=0).astype(jnp.bfloat16)
    copy.wait()
    total = own_part[...].astype(jnp.float32) + other_part[...].astype(jnp.float32)
    mixed = (tokens[...].astype(jnp.float32) + total).astype(jnp.bfloat16)
    mixed_out[...] = mixed
    normed = rms_scale(mixed, gain[...]).astype(jnp.bfloat16)
    normed_out[...] = normed
    wide = padded_rows(normed.astype(jnp.float32), 0.0)
    low = index[0] == 0
    stack = [
        jnp.where(
            low, wide[:, c * lanes : (c + 1) * lanes], wide[:, cols + c * lanes : cols + (c + 1) * lanes]
        )
        for c in range(chunks)
    ]
    stack = jnp.concatenate(stack, axis=0).astype(jnp.bfloat16)
    send = jnp.dot(picks, stack, preferred_element_type=jnp.float32).astype(jnp.bfloat16)
    for e in range(experts):
        send_out[e] = send[e * block : (e + 1) * block]


def shares_body(ids, weights, after, high_out, low_out):
    experts, padded, block = high_out.shape
    chunks = padded // 8
    seq_dev, top_count = ids.shape
    cap = capacity_of(seq_dev, top_count, experts)
    codes = padded_rows(slot_codes(ids[...], experts), -1.0)
    expert = lax.broadcasted_iota(jnp.int32, (seq_dev, experts), 1)
    shares = jnp.zeros((seq_dev, experts), jnp.float32)
    for k in range(top_count):
        shares = shares + jnp.where(ids[:, k : k + 1] == expert, weights[:, k : k + 1], 0.0)
    codes = jnp.concatenate([codes] * chunks, axis=0)
    shares = jnp.concatenate([padded_rows(shares, 0.0)] * chunks, axis=0)
    rank, _ = slot_map((padded, block), cap, 1, 0)
    for e in range(experts):
        share = jnp.where(codes[:, e : e + 1] == rank, shares[:, e : e + 1], 0.0)
        high = share.astype(jnp.bfloat16)
        high_out[e] = high
        low_out[e] = (share - high.astype(jnp.float32)).astype(jnp.bfloat16)


def expert_body(
    index, own, other, gate_hbm, up_hbm, down_hbm, own_out, sent_out, rows, gate, up, down, sems
):
    pairs = ((gate_hbm, gate), (up_hbm, up), (down_hbm, down))
    copies = [pltpu.make_async_copy(a, b, sems.at[i]) for i, (a, b) in enumerate(pairs)]
    copies[0].start()
    copies[1].start()
    experts, block, lanes = own.shape
    cols = rows.shape[1] // 2
    chunks = cols // lanes
    cap = block_cap(block, chunks)
    tp = index[0]
    rank, place = slot_map((chunks * 8, block), cap, 1, 0)
    spread = jnp.where(rank == place, 1.0, 0.0).astype(jnp.bfloat16)
    rank, place = slot_map((block, chunks * 8), cap, 0, 1)
    gather = jnp.where(rank == place, 1.0, 0.0).astype(jnp.bfloat16)
    for source, half in ((own, tp), (other, 1 - tp)):
        start = half * cols
        for e in range(experts):
            got = jnp.dot(spread, source[e], preferred_element_type=jnp.float32)
            for c in range(chunks):
                at = pl.ds(pl.multiple_of(start + c * lanes, lanes), lanes)
                rows[e * 8 : (e + 1) * 8, at] = got[c * 8 : (c + 1) * 8]
    copies[2].start()
    x = rows[...].astype(jnp.bfloat16)
    copies[0].wait()
    gate_part = jnp.dot(x, gate[...], preferred_element_type=jnp.float32)
    copies[1].wait()
    up_part = jnp.dot(x, up[...], preferred_element_type=jnp.float32)
    hidden = (gate_part / (1.0 + jnp.exp(-gate_part)) * up_part).astype(jnp.bfloat16)
    copies[2].wait()
    rows[...] = jnp.dot(hidden, down[...], preferred_element_type=jnp.float32)
    for target, half in ((sent_out, 1 - tp), (own_out, tp)):
        start = half * cols
        for e in range(experts):
            tiles = [
                rows[e * 8 : (e + 1) * 8, pl.ds(pl.multiple_of(start + c * lanes, lanes), lanes)]
                for c in range(chunks)
            ]
            tiles = jnp.concatenate(tiles, axis=0).astype(jnp.bfloat16)
            packed = jnp.dot(gather, tiles, preferred_element_type=jnp.float32)
            target[e] = packed.astype(jnp.bfloat16)


def combine_body(index, returned, high, low, mixed, own_shared, other_shared, result):
    experts, block, lanes = returned.shape
    cols = result.shape[1]
    seq_dev = result.shape[0]
    acc = jnp.zeros((high.shape[1], lanes), jnp.float32)
    for e in range(experts):
        acc = acc + jnp.dot(high[e], returned[e], preferred_element_type=jnp.float32)
        acc = acc + jnp.dot(low[e], returned[e], preferred_element_type=jnp.float32)
    first = index[0] == 0
    for c in range(cols // lanes):
        left = slice(c * lanes, (c + 1) * lanes)
        right = slice(cols + c * lanes, cols + (c + 1) * lanes)
        kept = jnp.where(first, mixed[:, left].astype(jnp.float32), mixed[:, right].astype(jnp.float32))
        own = jnp.where(
            first, own_shared[:, left].astype(jnp.float32), own_shared[:, right].astype(jnp.float32)
        )
        shared = own + other_shared[:, left].astype(jnp.float32)
        total = kept + acc[c * 8 : c * 8 + seq_dev] + shared
        result[:, left] = total.astype(jnp.bfloat16)


def capacity_of(seq_dev, top_count, experts):
    return min(seq_dev, max(2, 2 * seq_dev * top_count // experts))


def block_cap(block, chunks):
    return block // chunks


def routed_pair(
    tokens,
    attn_part,
    moe_gain,
    gate_weight,
    up_weight,
    down_weight,
    shared_gate,
    shared_up,
    shared_down,
    expert_ids,
    expert_weights,
):
    seq_dev, model_width = tokens.shape
    experts = lax.axis_size("ep")
    cols = model_width // 2
    lanes = 128
    chunks = cols // lanes
    cap = capacity_of(seq_dev, expert_ids.shape[1], experts)
    block = (cap * chunks + 15) // 16 * 16
    bf16 = jnp.bfloat16
    vmem = pl.BlockSpec(memory_space=pltpu.VMEM)
    smem = pl.BlockSpec(memory_space=pltpu.SMEM)
    anywhere = pl.BlockSpec(memory_space=pltpu.HBM)
    swap = [(0, 1), (1, 0)]
    index = lax.axis_index("tp").astype(jnp.int32).reshape(1)
    other_part = lax.ppermute(attn_part, "tp", swap)
    shape = jax.ShapeDtypeStruct
    packed = shape((experts, block, lanes), bf16)
    rows = shape((seq_dev, model_width), bf16)
    mixed, normed, send = pl.pallas_call(
        prepare_body,
        out_shape=(rows, rows, packed),
        in_specs=[smem, vmem, anywhere] + [vmem] * 3,
        out_specs=(vmem,) * 3,
        scratch_shapes=[pltpu.VMEM((seq_dev, model_width), bf16), pltpu.SemaphoreType.DMA],
        compiler_params=pltpu.CompilerParams(vmem_limit_bytes=8 << 20),
        name="prepare",
    )(index, tokens, attn_part, other_part, moe_gain.reshape(1, -1), expert_ids)
    arrived = lax.all_to_all(send, "ep", split_axis=0, concat_axis=0, tiled=True)
    hidden = gate_weight.shape[2]
    mix = shape((experts, chunks * 8, block), bf16)
    high, low = pl.pallas_call(
        shares_body,
        out_shape=(mix, mix),
        in_specs=[vmem, vmem, anywhere],
        out_specs=(vmem,) * 2,
        compiler_params=pltpu.CompilerParams(vmem_limit_bytes=8 << 20),
        cost_estimate=pl.CostEstimate(
            flops=SHARES_FLOPS, transcendentals=0, bytes_accessed=4 * experts * chunks * 8 * block
        ),
        name="shares",
    )(expert_ids, expert_weights, normed)
    arrived, high = lax.optimization_barrier((arrived, high))
    partner = lax.ppermute(arrived, "tp", swap)
    own_out, sent_out = pl.pallas_call(
        expert_body,
        out_shape=(packed, packed),
        in_specs=[smem] + [vmem] * 2 + [anywhere] * 3,
        out_specs=(vmem,) * 2,
        scratch_shapes=[
            pltpu.VMEM((experts * 8, model_width), jnp.float32),
            pltpu.VMEM((model_width, hidden), bf16),
            pltpu.VMEM((model_width, hidden), bf16),
            pltpu.VMEM((hidden, model_width), bf16),
            pltpu.SemaphoreType.DMA((3,)),
        ],
        compiler_params=pltpu.CompilerParams(vmem_limit_bytes=24 << 20),
        name="expert",
    )(
        index,
        arrived,
        partner,
        *(
            pltpu.with_memory_space_constraint(weight[0], pltpu.HBM)
            for weight in (gate_weight, up_weight, down_weight)
        ),
    )
    expert_sum = own_out.astype(jnp.float32) + lax.ppermute(sent_out, "tp", swap).astype(jnp.float32)
    returned = lax.all_to_all(
        expert_sum.astype(bf16), "ep", split_axis=0, concat_axis=0, tiled=True
    )
    shared_gate_out = jnp.dot(normed, shared_gate, preferred_element_type=jnp.float32)
    shared_up_out = jnp.dot(normed, shared_up, preferred_element_type=jnp.float32)
    shared_hidden = (jax.nn.silu(shared_gate_out) * shared_up_out).astype(bf16)
    shared_part = jnp.dot(shared_hidden, shared_down, preferred_element_type=jnp.float32)
    shared_part = shared_part.astype(bf16)
    shared_sent = lax.dynamic_slice_in_dim(shared_part, (1 - index[0]) * cols, cols, 1)
    shared_other = lax.ppermute(shared_sent, "tp", swap)
    return pl.pallas_call(
        combine_body,
        out_shape=shape((seq_dev, cols), bf16),
        in_specs=[smem] + [vmem] * 6,
        out_specs=vmem,
        compiler_params=pltpu.CompilerParams(vmem_limit_bytes=8 << 20),
        name="combine",
    )(index, returned, high, low, mixed, shared_part, shared_other)


def attend_plain(
    tokens,
    attn_gain,
    query_weight,
    key_weight,
    value_weight,
    out_weight,
    lambdas,
    head_gain,
    cache_keys,
    cache_values,
    lengths,
):
    seq_dev, model_width = tokens.shape
    local_heads = lambdas.shape[0]
    head_dim = cache_keys.shape[-1] // 2
    cache_len = cache_keys.shape[1]
    normed = rms_scale(tokens, attn_gain).astype(jnp.bfloat16)
    query_rows = jnp.dot(normed, query_weight, preferred_element_type=jnp.float32).astype(
        jnp.bfloat16
    )
    key_new = jnp.dot(normed, key_weight, preferred_element_type=jnp.float32).astype(jnp.bfloat16)
    value_new = jnp.dot(normed, value_weight, preferred_element_type=jnp.float32).astype(
        jnp.bfloat16
    )
    score_scale = head_dim ** (-0.5)
    queries = query_rows.reshape(seq_dev, local_heads, 2, head_dim)
    new_keys = key_new.reshape(seq_dev, local_heads, 2, head_dim)
    new_values = value_new.reshape(seq_dev, local_heads, 2 * head_dim)
    past_keys = cache_keys.reshape(seq_dev, cache_len, local_heads, 2, head_dim)
    scores = (
        jnp.einsum("shmd,sjhmd->shmj", queries, past_keys, preferred_element_type=jnp.float32)
        * score_scale
    )
    own_score = (
        jnp.sum(queries.astype(jnp.float32) * new_keys.astype(jnp.float32), axis=-1) * score_scale
    )
    live_mask = (jnp.arange(cache_len, dtype=jnp.int32)[None, :] < lengths[:, None])[
        :, None, None, :
    ]
    peak_score = jnp.maximum(jnp.max(jnp.where(live_mask, scores, -jnp.inf), axis=-1), own_score)
    exp_terms = jnp.where(live_mask, jnp.exp(scores - peak_score[..., None]), 0.0)
    own_term = jnp.exp(own_score - peak_score)
    denom_sum = jnp.sum(exp_terms, axis=-1) + own_term
    map_probs = exp_terms / denom_sum[..., None]
    own_prob = own_term / denom_sum
    lambda_row = lambdas[None, :]
    mixture = (map_probs[:, :, 0] - lambda_row[..., None] * map_probs[:, :, 1]).astype(jnp.bfloat16)
    own_mixture = (own_prob[:, :, 0] - lambda_row * own_prob[:, :, 1]).astype(jnp.bfloat16)
    head_out = jnp.einsum(
        "shj,sjhv->shv", mixture, cache_values, preferred_element_type=jnp.float32
    )
    head_out = head_out + own_mixture.astype(jnp.float32)[..., None] * new_values.astype(
        jnp.float32
    )
    head_normed = (
        rms_scale(head_out, head_gain)
        .astype(jnp.bfloat16)
        .reshape(seq_dev, local_heads * 2 * head_dim)
    )
    return lax.dot_general(
        head_normed, out_weight, (((1,), (1,)), ((), ())), preferred_element_type=jnp.float32
    ).astype(jnp.bfloat16)


def scatter_sum(part):
    part = part.astype(jnp.bfloat16)
    if lax.axis_size("tp") != 2:
        return lax.psum_scatter(part, "tp", scatter_dimension=1, tiled=True).astype(jnp.float32)
    cols = part.shape[1] // 2
    index = lax.axis_index("tp")
    own = lax.dynamic_slice_in_dim(part, index * cols, cols, 1)
    sent = lax.dynamic_slice_in_dim(part, (1 - index) * cols, cols, 1)
    arrived = lax.ppermute(sent, "tp", [(0, 1), (1, 0)])
    return own.astype(jnp.float32) + arrived.astype(jnp.float32)


def shards(
    tokens,
    attn_gain,
    query_weight,
    key_weight,
    value_weight,
    out_weight,
    lambdas,
    head_gain,
    cache_keys,
    cache_values,
    lengths,
    moe_gain,
    gate_weight,
    up_weight,
    down_weight,
    shared_gate,
    shared_up,
    shared_down,
    expert_ids,
    expert_weights,
):
    seq_dev, model_width = tokens.shape
    cache_len, local_heads = cache_keys.shape[1:3]
    pair = lax.axis_size("tp") == 2 and model_width % 256 == 0 and seq_dev <= 8
    pair = pair and cache_len % STEP == 0 and STEP * local_heads % (2 * CHUNK) == 0
    attend = attend_kernel if pair else attend_plain
    attn_part = attend(
        tokens,
        attn_gain,
        query_weight,
        key_weight,
        value_weight,
        out_weight,
        lambdas,
        head_gain,
        cache_keys,
        cache_values,
        lengths,
    )
    if pair:
        return routed_pair(
            tokens,
            attn_part,
            moe_gain,
            gate_weight,
            up_weight,
            down_weight,
            shared_gate,
            shared_up,
            shared_down,
            expert_ids,
            expert_weights,
        )
    attn_total = lax.psum(attn_part, "tp").astype(jnp.float32)
    mixed_rows = (tokens.astype(jnp.float32) + attn_total).astype(jnp.bfloat16)
    moe_normed = rms_scale(mixed_rows, moe_gain).astype(jnp.bfloat16)
    shared_gate_out = jnp.dot(moe_normed, shared_gate, preferred_element_type=jnp.float32)
    shared_up_out = jnp.dot(moe_normed, shared_up, preferred_element_type=jnp.float32)
    shared_hidden = (jax.nn.silu(shared_gate_out) * shared_up_out).astype(jnp.bfloat16)
    shared_part = jnp.dot(shared_hidden, shared_down, preferred_element_type=jnp.float32)
    experts = lax.axis_size("ep")
    top_count = expert_ids.shape[1]
    capacity = min(seq_dev, max(2, 2 * seq_dev * top_count // experts))
    slot_count = seq_dev * top_count
    slot_ids = expert_ids.reshape(slot_count)
    expert_hits = (slot_ids[:, None] == jnp.arange(experts, dtype=jnp.int32)[None, :]).astype(
        jnp.int32
    )
    slot_rank = jnp.sum((jnp.cumsum(expert_hits, axis=0) - expert_hits) * expert_hits, axis=1)
    slot_place = slot_ids * capacity + slot_rank
    placed = (
        slot_place[:, None] == jnp.arange(experts * capacity, dtype=jnp.int32)[None, :]
    ).astype(jnp.bfloat16)
    slot_token = jnp.arange(slot_count, dtype=jnp.int32) // top_count
    token_pick = (slot_token[:, None] == jnp.arange(seq_dev, dtype=jnp.int32)[None, :]).astype(
        jnp.bfloat16
    )
    dispatch = lax.dot_general(
        placed, token_pick, (((0,), (0,)), ((), ())), preferred_element_type=jnp.float32
    ).astype(jnp.bfloat16)
    col_count = model_width // lax.axis_size("tp")
    own_start = lax.axis_index("tp") * col_count
    own_normed = lax.dynamic_slice_in_dim(moe_normed, own_start, col_count, 1)
    send_slice = jnp.dot(dispatch, own_normed, preferred_element_type=jnp.float32).astype(
        jnp.bfloat16
    )
    arrived = lax.all_to_all(send_slice, "ep", split_axis=0, concat_axis=0, tiled=True)
    received = lax.all_gather(arrived, "tp", axis=1, tiled=True)
    gate_out = jnp.dot(received, gate_weight[0], preferred_element_type=jnp.float32)
    up_out = jnp.dot(received, up_weight[0], preferred_element_type=jnp.float32)
    expert_hidden = (jax.nn.silu(gate_out) * up_out).astype(jnp.bfloat16)
    expert_part = jnp.dot(expert_hidden, down_weight[0], preferred_element_type=jnp.float32)
    expert_sum, shared_out = scatter_sum(expert_part), scatter_sum(shared_part)
    returned = lax.all_to_all(
        expert_sum.astype(jnp.bfloat16), "ep", split_axis=0, concat_axis=0, tiled=True
    )
    slot_values = jnp.dot(placed, returned, preferred_element_type=jnp.float32).reshape(
        seq_dev, top_count, col_count
    )
    routed = jnp.sum(expert_weights[:, :, None] * slot_values, axis=1)
    own_cols = lax.dynamic_slice_in_dim(mixed_rows, own_start, col_count, 1)
    return (own_cols.astype(jnp.float32) + routed + shared_out).astype(jnp.bfloat16)


def solution(mesh):
    in_specs = (
        P("ep", None),
        P(),
        P(None, "tp"),
        P(None, "tp"),
        P(None, "tp"),
        P(None, "tp"),
        P("tp"),
        P(),
        P("ep", None, "tp", None),
        P("ep", None, "tp", None),
        P("ep"),
        P(),
        P("ep", None, "tp"),
        P("ep", None, "tp"),
        P("ep", "tp", None),
        P(None, "tp"),
        P(None, "tp"),
        P("tp", None),
        P("ep", None),
        P("ep", None),
    )
    out_specs = P("ep", "tp")
    return jax.shard_map(shards, mesh=mesh, in_specs=in_specs, out_specs=out_specs, check_vma=False)
```

```python
import jax
import jax.numpy as jnp
from jax import lax
from jax.experimental import pallas as pl
from jax.experimental.pallas import tpu as pltpu
from jax.sharding import PartitionSpec as P

epsilon = 1e-06
GRAIN = 128
STEP = 256
CHUNK = 1024
PIECES = 1
FLIGHT = 3
AHEAD = 7
OUT_AT = 1
SHARES_FLOPS = 4_000_000_000


def rms_scale(values, gain):
    wide = values.astype(jnp.float32)
    return (
        wide
        * lax.rsqrt(jnp.mean(wide * wide, axis=-1, keepdims=True) + epsilon)
        * gain.astype(jnp.float32)
    )


def attend_body(
    lengths_hbm,
    lambdas_hbm,
    tokens_hbm,
    attn_gain_hbm,
    head_gain_hbm,
    query_hbm,
    key_hbm,
    value_hbm,
    out_hbm,
    keys_hbm,
    values_hbm,
    part_out,
    lengths,
    lambdas,
    tokens,
    attn_gain,
    head_gain,
    query_w,
    key_w,
    value_w,
    out_w,
    keys,
    values,
    scores,
    peaks,
    own_scores,
    queries,
    new_keys,
    new_values,
    head_outs,
    head_rows,
    small_sems,
    weight_sems,
    key_sems,
    value_sems,
):
    seq_dev = tokens.shape[0]
    heads = queries.shape[1]
    width = queries.shape[2]
    head_dim = width // 2
    cache_rows = keys.shape[1]
    scale = head_dim ** (-0.5)
    grain_rows = GRAIN * heads
    span = query_w.shape[0] // PIECES

    def weight_copy(i, piece):
        source = (query_hbm, key_hbm, value_hbm, out_hbm)[i]
        target = (query_w, key_w, value_w, out_w)[i]
        rows = pl.ds(piece * span, span)
        return pltpu.make_async_copy(source.at[rows], target.at[rows], weight_sems.at[i, piece])

    def live_rows(s):
        return pl.multiple_of((lengths[s] + GRAIN - 1) // GRAIN * grain_rows, grain_rows)

    def key_copy(s):
        rows = pl.ds(0, live_rows(s))
        return pltpu.make_async_copy(keys_hbm.at[s, rows], keys.at[s, rows], key_sems.at[s])

    def value_copy(s):
        rows = pl.ds(0, live_rows(s))
        return pltpu.make_async_copy(values_hbm.at[s, rows], values.at[s, rows], value_sems.at[s])

    small = [
        pltpu.make_async_copy(source, target, small_sems.at[i])
        for i, (source, target) in enumerate(
            (
                (lengths_hbm, lengths),
                (lambdas_hbm, lambdas),
                (tokens_hbm, tokens),
                (attn_gain_hbm, attn_gain),
                (head_gain_hbm, head_gain),
            )
        )
    ]
    for copy in small:
        copy.start()
    queue = [(weight_copy, (i, piece)) for i in range(3) for piece in range(PIECES)]
    for s in range(AHEAD):
        queue += [(key_copy, (s,)), (value_copy, (s,))]

    def start_next():
        if queue:
            make, where = queue.pop(0)
            make(*where).start()

    for _ in range(FLIGHT):
        start_next()
    for copy in small:
        copy.wait()

    def clear_tail(s, carry):
        def clear(g, carry):
            rows = pl.ds(pl.multiple_of(g * grain_rows, grain_rows), grain_rows)
            keys[s, rows, :] = jnp.zeros((grain_rows, width), jnp.bfloat16)
            values[s, rows, :] = jnp.zeros((grain_rows, width), jnp.bfloat16)
            return carry

        used = (lengths[s] + STEP - 1) // STEP * STEP * heads
        return lax.fori_loop(live_rows(s) // grain_rows, used // grain_rows, clear, carry)

    lax.fori_loop(0, seq_dev, clear_tail, 0)

    normed = rms_scale(tokens[...], attn_gain[...].astype(jnp.float32).reshape(1, -1)).astype(jnp.bfloat16)
    for i, (weight, target) in enumerate(
        ((query_w, queries), (key_w, new_keys), (value_w, new_values))
    ):
        rows = None
        for piece in range(PIECES):
            weight_copy(i, piece).wait()
            start_next()
            lines = slice(piece * span, (piece + 1) * span)
            more = jnp.dot(normed[:, lines], weight[lines, :], preferred_element_type=jnp.float32)
            rows = more if rows is None else rows + more
        rows = rows.astype(jnp.bfloat16).astype(jnp.float32)
        for s in range(seq_dev):
            for h in range(heads):
                target[s, h : h + 1, :] = rows[s : s + 1, h * width : (h + 1) * width]

    while queue:
        start_next()
    lane = lax.broadcasted_iota(jnp.int32, (2 * heads, width), 1)
    row = lax.broadcasted_iota(jnp.int32, (2 * heads, width), 0)
    map_mask = (lane < head_dim) == (row < heads)
    lane_or_far = jnp.where(lane % heads == row % heads, lane, jnp.int32(1 << 30))
    head_row = lax.broadcasted_iota(jnp.int32, (heads, 1), 0)
    lam = jnp.zeros((heads, 1), jnp.float32)
    for h in range(heads):
        lam = jnp.where(head_row == h, lambdas[h], lam)

    def score_stage(s, size):
        slot = s % 2
        live = lengths[s] * heads
        query = queries[s]
        query16 = jnp.where(map_mask, jnp.concatenate([query, query], axis=0), 0.0)
        fresh = new_keys[s]
        fresh16 = jnp.concatenate([fresh, fresh], axis=0)
        own = jnp.sum(query16 * fresh16, axis=1, keepdims=True) * scale
        query16 = (query16 * scale).astype(jnp.bfloat16)
        none = jnp.zeros_like(query16)
        query32 = jnp.concatenate(
            [
                jnp.concatenate([query16, none], axis=1),
                jnp.concatenate([none, query16], axis=1),
            ],
            axis=0,
        )
        half = size * heads // 2
        peak = jnp.full((2 * heads, width), -jnp.inf, jnp.float32)
        for c in range(0, half, CHUNK):
            pair = jnp.concatenate(
                [keys[s, c : c + CHUNK, :], keys[s, half + c : half + c + CHUNK, :]], axis=1
            )
            block = lax.dot_general(
                query32, pair, (((1,), (1,)), ((), ())), preferred_element_type=jnp.float32
            )
            for part in range(2):
                for j in range(0, CHUNK, width):
                    start = part * half + c + j
                    tile = block[part * 2 * heads : (part + 1) * 2 * heads, j : j + width]
                    tile = jnp.where(lane_or_far < live - start, tile, -jnp.inf)
                    scores[slot, :, start : start + width] = tile
                    peak = jnp.maximum(peak, tile)
        peak = jnp.maximum(jnp.max(peak, axis=1, keepdims=True), own)
        peaks[slot] = jnp.broadcast_to(peak, (2 * heads, width))
        own_scores[slot] = jnp.broadcast_to(own, (2 * heads, width))

    def value_stage(s, size):
        slot = s % 2
        rows = size * heads
        half = rows // 2
        peak = peaks[slot]
        own_term = jnp.exp(own_scores[slot] - peak)
        sums = [jnp.zeros((2 * heads, width), jnp.float32) for _ in range(4)]
        for i, start in enumerate(range(0, rows, width)):
            tile = jnp.exp(scores[slot, :, start : start + width] - peak)
            scores[slot, :, start : start + width] = tile
            sums[i % 4] = sums[i % 4] + tile
        total = (sums[0] + sums[1]) + (sums[2] + sums[3])
        inverse = 1.0 / (jnp.sum(total, axis=1, keepdims=True) + own_term)
        first = inverse[:heads]
        second = lam * inverse[heads:]
        acc = jnp.zeros((2 * heads, 2 * width), jnp.float32)
        for c in range(0, half, CHUNK):
            tiles = []
            for j in range(c, c + CHUNK, width):
                mixed = [
                    scores[slot, :heads, start : start + width] * first
                    - scores[slot, heads:, start : start + width] * second
                    for start in (j, half + j)
                ]
                tiles.append(jnp.concatenate(mixed, axis=0).astype(jnp.bfloat16))
            pair = jnp.concatenate(
                [values[s, c : c + CHUNK, :], values[s, half + c : half + c + CHUNK, :]], axis=1
            )
            acc = acc + jnp.dot(
                jnp.concatenate(tiles, axis=1), pair, preferred_element_type=jnp.float32
            )
        own_mixture = own_term[:heads] * first - own_term[heads:] * second
        own_mixture = own_mixture.astype(jnp.bfloat16).astype(jnp.float32)
        head_outs[s] = acc[:heads, :width] + acc[heads:, width:] + own_mixture * new_values[s]

    full = cache_rows // heads
    sizes = tuple(range(STEP, full + 1, STEP))

    def sized(run, s):
        for size in sizes:

            @pl.when((lengths[s] > size - STEP) & (lengths[s] <= size))
            def _():
                run(s, size)

    key_copy(0).wait()
    sized(score_stage, 0)

    def stage(s, carry):
        key_copy(s).wait()
        value_copy(s - 1).wait()

        @pl.when(s + AHEAD - 1 < seq_dev)
        def _():
            key_copy(s + AHEAD - 1).start()
            value_copy(s + AHEAD - 1).start()

        @pl.when(s == OUT_AT)
        def _():
            for piece in range(PIECES):
                weight_copy(3, piece).start()

        sized(score_stage, s)
        sized(value_stage, s - 1)
        return carry

    lax.fori_loop(1, seq_dev, stage, 0)
    value_copy(seq_dev - 1).wait()
    sized(value_stage, seq_dev - 1)
    head_normed = rms_scale(head_outs[...], head_gain[...].reshape(1, 1, width))
    for s in range(seq_dev):
        for h in range(heads):
            head_rows[s : s + 1, h * width : (h + 1) * width] = head_normed[s, h : h + 1, :]
    for piece in range(PIECES):
        weight_copy(3, piece).wait()
    part = lax.dot_general(
        head_rows[:seq_dev, :].astype(jnp.bfloat16),
        out_w[...],
        (((1,), (1,)), ((), ())),
        preferred_element_type=jnp.float32,
    )
    part_out[...] = part.astype(jnp.bfloat16)


def attend_kernel(
    tokens,
    attn_gain,
    query_weight,
    key_weight,
    value_weight,
    out_weight,
    lambdas,
    head_gain,
    cache_keys,
    cache_values,
    lengths,
):
    seq_dev, model_width = tokens.shape
    _, cache_len, heads, width = cache_keys.shape
    cols = heads * width
    rows = cache_len * heads
    vmem = pl.BlockSpec(memory_space=pltpu.VMEM)
    anywhere = pl.BlockSpec(memory_space=pltpu.HBM)
    bf16, f32 = jnp.bfloat16, jnp.float32
    return pl.pallas_call(
        attend_body,
        out_shape=jax.ShapeDtypeStruct((seq_dev, model_width), bf16),
        in_specs=[anywhere] * 11,
        out_specs=vmem,
        scratch_shapes=[
            pltpu.SMEM((seq_dev,), jnp.int32),
            pltpu.SMEM((heads,), f32),
            pltpu.VMEM((seq_dev, model_width), bf16),
            pltpu.VMEM((model_width,), bf16),
            pltpu.VMEM((1, width), bf16),
            pltpu.VMEM((model_width, cols), bf16),
            pltpu.VMEM((model_width, cols), bf16),
            pltpu.VMEM((model_width, cols), bf16),
            pltpu.VMEM((model_width, cols), bf16),
            pltpu.VMEM((seq_dev, rows, width), bf16),
            pltpu.VMEM((seq_dev, rows, width), bf16),
            pltpu.VMEM((2, 2 * heads, rows), f32),
            pltpu.VMEM((2, 2 * heads, width), f32),
            pltpu.VMEM((2, 2 * heads, width), f32),
            pltpu.VMEM((seq_dev, heads, width), f32),
            pltpu.VMEM((seq_dev, heads, width), f32),
            pltpu.VMEM((seq_dev, heads, width), f32),
            pltpu.VMEM((seq_dev, heads, width), f32),
            pltpu.VMEM((seq_dev + 1, cols), f32),
            pltpu.SemaphoreType.DMA((5,)),
            pltpu.SemaphoreType.DMA((4, PIECES)),
            pltpu.SemaphoreType.DMA((seq_dev,)),
            pltpu.SemaphoreType.DMA((seq_dev,)),
        ],
        compiler_params=pltpu.CompilerParams(vmem_limit_bytes=54 << 20),
        name="attend",
    )(
        lengths,
        lambdas,
        tokens,
        attn_gain,
        head_gain.reshape(1, -1),
        query_weight,
        key_weight,
        value_weight,
        out_weight,
        cache_keys.reshape(seq_dev, rows, width),
        cache_values.reshape(seq_dev, rows, width),
    )


def slot_map(shape, cap, rows_at, slots_at):
    packed = lax.broadcasted_iota(jnp.int32, shape, rows_at)
    padded = lax.broadcasted_iota(jnp.int32, shape, slots_at)
    rank = jnp.full(shape, -7, jnp.int32)
    place = jnp.full(shape, -9, jnp.int32)
    for c in range(shape[slots_at] // 8):
        inside = (packed >= c * cap) & (packed < (c + 1) * cap)
        inside = inside & (padded >= c * 8) & (padded < (c + 1) * 8)
        rank = jnp.where(inside, packed - c * cap, rank)
        place = jnp.where(inside, padded - c * 8, place)
    return rank.astype(jnp.float32), place.astype(jnp.float32)


def slot_codes(ids, experts):
    seq_dev, top_count = ids.shape
    expert = lax.broadcasted_iota(jnp.int32, (seq_dev, experts), 1)
    hits = jnp.zeros((seq_dev, experts), jnp.float32)
    for k in range(top_count):
        hits = hits + jnp.where(ids[:, k : k + 1] == expert, 1.0, 0.0)
    earlier = lax.broadcasted_iota(jnp.int32, (seq_dev, seq_dev), 0)
    earlier = earlier > lax.broadcasted_iota(jnp.int32, (seq_dev, seq_dev), 1)
    rank = jnp.dot(
        jnp.where(earlier, 1.0, 0.0).astype(jnp.bfloat16),
        hits.astype(jnp.bfloat16),
        preferred_element_type=jnp.float32,
    )
    return jnp.where(hits > 0.5, rank, -1.0)


def padded_rows(rows, value):
    seq_dev, cols = rows.shape
    if seq_dev == 8:
        return rows
    return jnp.concatenate([rows, jnp.full((8 - seq_dev, cols), value, rows.dtype)], axis=0)


def prepare_body(
    index, tokens, own_hbm, other_part, gain, ids, mixed_out, normed_out, send_out, own_part, sem
):
    copy = pltpu.make_async_copy(own_hbm, own_part, sem)
    copy.start()
    experts, block, lanes = send_out.shape
    cols = tokens.shape[1] // 2
    chunks = cols // lanes
    cap = capacity_of(tokens.shape[0], ids.shape[1], experts)
    codes = padded_rows(slot_codes(ids[...], experts), -1.0)
    codes = jnp.concatenate([codes] * chunks, axis=0)
    expert = lax.broadcasted_iota(jnp.int32, (experts, experts), 0)
    eye = expert == lax.broadcasted_iota(jnp.int32, (experts, experts), 1)
    code_rows = lax.dot_general(
        jnp.where(eye, 1.0, 0.0).astype(jnp.bfloat16),
        codes.astype(jnp.bfloat16),
        (((1,), (1,)), ((), ())),
        preferred_element_type=jnp.float32,
    )
    rank, _ = slot_map((block, chunks * 8), cap, 0, 1)
    picks = [jnp.where(code_rows[e : e + 1, :] == rank, 1.0, 0.0) for e in range(experts)]
    picks = jnp.concatenate(picks, axis=0).astype(jnp.bfloat16)
    copy.wait()
    total = own_part[...].astype(jnp.float32) + other_part[...].astype(jnp.float32)
    mixed = (tokens[...].astype(jnp.float32) + total).astype(jnp.bfloat16)
    mixed_out[...] = mixed
    normed = rms_scale(mixed, gain[...]).astype(jnp.bfloat16)
    normed_out[...] = normed
    wide = padded_rows(normed.astype(jnp.float32), 0.0)
    low = index[0] == 0
    stack = [
        jnp.where(
            low, wide[:, c * lanes : (c + 1) * lanes], wide[:, cols + c * lanes : cols + (c + 1) * lanes]
        )
        for c in range(chunks)
    ]
    stack = jnp.concatenate(stack, axis=0).astype(jnp.bfloat16)
    send = jnp.dot(picks, stack, preferred_element_type=jnp.float32).astype(jnp.bfloat16)
    for e in range(experts):
        send_out[e] = send[e * block : (e + 1) * block]


def shares_body(ids, weights, after, high_out, low_out):
    experts, padded, block = high_out.shape
    chunks = padded // 8
    seq_dev, top_count = ids.shape
    cap = capacity_of(seq_dev, top_count, experts)
    codes = padded_rows(slot_codes(ids[...], experts), -1.0)
    expert = lax.broadcasted_iota(jnp.int32, (seq_dev, experts), 1)
    shares = jnp.zeros((seq_dev, experts), jnp.float32)
    for k in range(top_count):
        shares = shares + jnp.where(ids[:, k : k + 1] == expert, weights[:, k : k + 1], 0.0)
    codes = jnp.concatenate([codes] * chunks, axis=0)
    shares = jnp.concatenate([padded_rows(shares, 0.0)] * chunks, axis=0)
    rank, _ = slot_map((padded, block), cap, 1, 0)
    for e in range(experts):
        share = jnp.where(codes[:, e : e + 1] == rank, shares[:, e : e + 1], 0.0)
        high = share.astype(jnp.bfloat16)
        high_out[e] = high
        low_out[e] = (share - high.astype(jnp.float32)).astype(jnp.bfloat16)


def expert_body(
    index, own, other, gate_hbm, up_hbm, down_hbm, own_out, sent_out, rows, gate, up, down, sems
):
    pairs = ((gate_hbm, gate), (up_hbm, up), (down_hbm, down))
    copies = [pltpu.make_async_copy(a, b, sems.at[i]) for i, (a, b) in enumerate(pairs)]
    copies[0].start()
    copies[1].start()
    experts, block, lanes = own.shape
    cols = rows.shape[1] // 2
    chunks = cols // lanes
    cap = block_cap(block, chunks)
    tp = index[0]
    rank, place = slot_map((chunks * 8, block), cap, 1, 0)
    spread = jnp.where(rank == place, 1.0, 0.0).astype(jnp.bfloat16)
    rank, place = slot_map((block, chunks * 8), cap, 0, 1)
    gather = jnp.where(rank == place, 1.0, 0.0).astype(jnp.bfloat16)
    for source, half in ((own, tp), (other, 1 - tp)):
        start = half * cols
        for e in range(experts):
            got = jnp.dot(spread, source[e], preferred_element_type=jnp.float32)
            for c in range(chunks):
                at = pl.ds(pl.multiple_of(start + c * lanes, lanes), lanes)
                rows[e * 8 : (e + 1) * 8, at] = got[c * 8 : (c + 1) * 8]
    copies[2].start()
    x = rows[...].astype(jnp.bfloat16)
    copies[0].wait()
    gate_part = jnp.dot(x, gate[...], preferred_element_type=jnp.float32)
    copies[1].wait()
    up_part = jnp.dot(x, up[...], preferred_element_type=jnp.float32)
    hidden = (gate_part / (1.0 + jnp.exp(-gate_part)) * up_part).astype(jnp.bfloat16)
    copies[2].wait()
    rows[...] = jnp.dot(hidden, down[...], preferred_element_type=jnp.float32)
    for target, half in ((sent_out, 1 - tp), (own_out, tp)):
        start = half * cols
        for e in range(experts):
            tiles = [
                rows[e * 8 : (e + 1) * 8, pl.ds(pl.multiple_of(start + c * lanes, lanes), lanes)]
                for c in range(chunks)
            ]
            tiles = jnp.concatenate(tiles, axis=0).astype(jnp.bfloat16)
            packed = jnp.dot(gather, tiles, preferred_element_type=jnp.float32)
            target[e] = packed.astype(jnp.bfloat16)


def combine_body(index, returned, high, low, mixed, own_shared, other_shared, result):
    experts, block, lanes = returned.shape
    cols = result.shape[1]
    seq_dev = result.shape[0]
    acc = jnp.zeros((high.shape[1], lanes), jnp.float32)
    for e in range(experts):
        acc = acc + jnp.dot(high[e], returned[e], preferred_element_type=jnp.float32)
        acc = acc + jnp.dot(low[e], returned[e], preferred_element_type=jnp.float32)
    first = index[0] == 0
    for c in range(cols // lanes):
        left = slice(c * lanes, (c + 1) * lanes)
        right = slice(cols + c * lanes, cols + (c + 1) * lanes)
        kept = jnp.where(first, mixed[:, left].astype(jnp.float32), mixed[:, right].astype(jnp.float32))
        own = jnp.where(
            first, own_shared[:, left].astype(jnp.float32), own_shared[:, right].astype(jnp.float32)
        )
        shared = own + other_shared[:, left].astype(jnp.float32)
        total = kept + acc[c * 8 : c * 8 + seq_dev] + shared
        result[:, left] = total.astype(jnp.bfloat16)


def capacity_of(seq_dev, top_count, experts):
    return min(seq_dev, max(2, 2 * seq_dev * top_count // experts))


def block_cap(block, chunks):
    return block // chunks


def routed_pair(
    tokens,
    attn_part,
    moe_gain,
    gate_weight,
    up_weight,
    down_weight,
    shared_gate,
    shared_up,
    shared_down,
    expert_ids,
    expert_weights,
):
    seq_dev, model_width = tokens.shape
    experts = lax.axis_size("ep")
    cols = model_width // 2
    lanes = 128
    chunks = cols // lanes
    cap = capacity_of(seq_dev, expert_ids.shape[1], experts)
    block = (cap * chunks + 15) // 16 * 16
    bf16 = jnp.bfloat16
    vmem = pl.BlockSpec(memory_space=pltpu.VMEM)
    smem = pl.BlockSpec(memory_space=pltpu.SMEM)
    anywhere = pl.BlockSpec(memory_space=pltpu.HBM)
    swap = [(0, 1), (1, 0)]
    index = lax.axis_index("tp").astype(jnp.int32).reshape(1)
    other_part = lax.ppermute(attn_part, "tp", swap)
    shape = jax.ShapeDtypeStruct
    packed = shape((experts, block, lanes), bf16)
    rows = shape((seq_dev, model_width), bf16)
    mixed, normed, send = pl.pallas_call(
        prepare_body,
        out_shape=(rows, rows, packed),
        in_specs=[smem, vmem, anywhere] + [vmem] * 3,
        out_specs=(vmem,) * 3,
        scratch_shapes=[pltpu.VMEM((seq_dev, model_width), bf16), pltpu.SemaphoreType.DMA],
        compiler_params=pltpu.CompilerParams(vmem_limit_bytes=8 << 20),
        name="prepare",
    )(
        index,
        tokens,
        pltpu.with_memory_space_constraint(attn_part, pltpu.HBM),
        other_part,
        moe_gain.reshape(1, -1),
        expert_ids,
    )
    arrived = lax.all_to_all(send, "ep", split_axis=0, concat_axis=0, tiled=True)
    hidden = gate_weight.shape[2]
    mix = shape((experts, chunks * 8, block), bf16)
    high, low = pl.pallas_call(
        shares_body,
        out_shape=(mix, mix),
        in_specs=[vmem, vmem, anywhere],
        out_specs=(vmem,) * 2,
        compiler_params=pltpu.CompilerParams(vmem_limit_bytes=8 << 20),
        cost_estimate=pl.CostEstimate(
            flops=SHARES_FLOPS, transcendentals=0, bytes_accessed=4 * experts * chunks * 8 * block
        ),
        name="shares",
    )(expert_ids, expert_weights, normed)
    arrived, high = lax.optimization_barrier((arrived, high))
    partner = lax.ppermute(arrived, "tp", swap)
    own_out, sent_out = pl.pallas_call(
        expert_body,
        out_shape=(packed, packed),
        in_specs=[smem] + [vmem] * 2 + [anywhere] * 3,
        out_specs=(vmem,) * 2,
        scratch_shapes=[
            pltpu.VMEM((experts * 8, model_width), jnp.float32),
            pltpu.VMEM((model_width, hidden), bf16),
            pltpu.VMEM((model_width, hidden), bf16),
            pltpu.VMEM((hidden, model_width), bf16),
            pltpu.SemaphoreType.DMA((3,)),
        ],
        compiler_params=pltpu.CompilerParams(vmem_limit_bytes=24 << 20),
        name="expert",
    )(
        index,
        arrived,
        partner,
        *(
            pltpu.with_memory_space_constraint(weight[0], pltpu.HBM)
            for weight in (gate_weight, up_weight, down_weight)
        ),
    )
    expert_sum = own_out.astype(jnp.float32) + lax.ppermute(sent_out, "tp", swap).astype(jnp.float32)
    returned = lax.all_to_all(
        expert_sum.astype(bf16), "ep", split_axis=0, concat_axis=0, tiled=True
    )
    shared_gate_out = jnp.dot(normed, shared_gate, preferred_element_type=jnp.float32)
    shared_up_out = jnp.dot(normed, shared_up, preferred_element_type=jnp.float32)
    shared_hidden = (jax.nn.silu(shared_gate_out) * shared_up_out).astype(bf16)
    shared_part = jnp.dot(shared_hidden, shared_down, preferred_element_type=jnp.float32)
    shared_part = shared_part.astype(bf16)
    shared_sent = lax.dynamic_slice_in_dim(shared_part, (1 - index[0]) * cols, cols, 1)
    shared_other = lax.ppermute(shared_sent, "tp", swap)
    return pl.pallas_call(
        combine_body,
        out_shape=shape((seq_dev, cols), bf16),
        in_specs=[smem] + [vmem] * 6,
        out_specs=vmem,
        compiler_params=pltpu.CompilerParams(vmem_limit_bytes=8 << 20),
        name="combine",
    )(index, returned, high, low, mixed, shared_part, shared_other)


def attend_plain(
    tokens,
    attn_gain,
    query_weight,
    key_weight,
    value_weight,
    out_weight,
    lambdas,
    head_gain,
    cache_keys,
    cache_values,
    lengths,
):
    seq_dev, model_width = tokens.shape
    local_heads = lambdas.shape[0]
    head_dim = cache_keys.shape[-1] // 2
    cache_len = cache_keys.shape[1]
    normed = rms_scale(tokens, attn_gain).astype(jnp.bfloat16)
    query_rows = jnp.dot(normed, query_weight, preferred_element_type=jnp.float32).astype(
        jnp.bfloat16
    )
    key_new = jnp.dot(normed, key_weight, preferred_element_type=jnp.float32).astype(jnp.bfloat16)
    value_new = jnp.dot(normed, value_weight, preferred_element_type=jnp.float32).astype(
        jnp.bfloat16
    )
    score_scale = head_dim ** (-0.5)
    queries = query_rows.reshape(seq_dev, local_heads, 2, head_dim)
    new_keys = key_new.reshape(seq_dev, local_heads, 2, head_dim)
    new_values = value_new.reshape(seq_dev, local_heads, 2 * head_dim)
    past_keys = cache_keys.reshape(seq_dev, cache_len, local_heads, 2, head_dim)
    scores = (
        jnp.einsum("shmd,sjhmd->shmj", queries, past_keys, preferred_element_type=jnp.float32)
        * score_scale
    )
    own_score = (
        jnp.sum(queries.astype(jnp.float32) * new_keys.astype(jnp.float32), axis=-1) * score_scale
    )
    live_mask = (jnp.arange(cache_len, dtype=jnp.int32)[None, :] < lengths[:, None])[
        :, None, None, :
    ]
    peak_score = jnp.maximum(jnp.max(jnp.where(live_mask, scores, -jnp.inf), axis=-1), own_score)
    exp_terms = jnp.where(live_mask, jnp.exp(scores - peak_score[..., None]), 0.0)
    own_term = jnp.exp(own_score - peak_score)
    denom_sum = jnp.sum(exp_terms, axis=-1) + own_term
    map_probs = exp_terms / denom_sum[..., None]
    own_prob = own_term / denom_sum
    lambda_row = lambdas[None, :]
    mixture = (map_probs[:, :, 0] - lambda_row[..., None] * map_probs[:, :, 1]).astype(jnp.bfloat16)
    own_mixture = (own_prob[:, :, 0] - lambda_row * own_prob[:, :, 1]).astype(jnp.bfloat16)
    head_out = jnp.einsum(
        "shj,sjhv->shv", mixture, cache_values, preferred_element_type=jnp.float32
    )
    head_out = head_out + own_mixture.astype(jnp.float32)[..., None] * new_values.astype(
        jnp.float32
    )
    head_normed = (
        rms_scale(head_out, head_gain)
        .astype(jnp.bfloat16)
        .reshape(seq_dev, local_heads * 2 * head_dim)
    )
    return lax.dot_general(
        head_normed, out_weight, (((1,), (1,)), ((), ())), preferred_element_type=jnp.float32
    ).astype(jnp.bfloat16)


def scatter_sum(part):
    part = part.astype(jnp.bfloat16)
    if lax.axis_size("tp") != 2:
        return lax.psum_scatter(part, "tp", scatter_dimension=1, tiled=True).astype(jnp.float32)
    cols = part.shape[1] // 2
    index = lax.axis_index("tp")
    own = lax.dynamic_slice_in_dim(part, index * cols, cols, 1)
    sent = lax.dynamic_slice_in_dim(part, (1 - index) * cols, cols, 1)
    arrived = lax.ppermute(sent, "tp", [(0, 1), (1, 0)])
    return own.astype(jnp.float32) + arrived.astype(jnp.float32)


def shards(
    tokens,
    attn_gain,
    query_weight,
    key_weight,
    value_weight,
    out_weight,
    lambdas,
    head_gain,
    cache_keys,
    cache_values,
    lengths,
    moe_gain,
    gate_weight,
    up_weight,
    down_weight,
    shared_gate,
    shared_up,
    shared_down,
    expert_ids,
    expert_weights,
):
    seq_dev, model_width = tokens.shape
    cache_len, local_heads = cache_keys.shape[1:3]
    pair = lax.axis_size("tp") == 2 and model_width % 256 == 0 and seq_dev <= 8
    pair = pair and cache_len % STEP == 0 and STEP * local_heads % (2 * CHUNK) == 0
    attend = attend_kernel if pair else attend_plain
    attn_part = attend(
        tokens,
        attn_gain,
        query_weight,
        key_weight,
        value_weight,
        out_weight,
        lambdas,
        head_gain,
        cache_keys,
        cache_values,
        lengths,
    )
    if pair:
        return routed_pair(
            tokens,
            attn_part,
            moe_gain,
            gate_weight,
            up_weight,
            down_weight,
            shared_gate,
            shared_up,
            shared_down,
            expert_ids,
            expert_weights,
        )
    attn_total = lax.psum(attn_part, "tp").astype(jnp.float32)
    mixed_rows = (tokens.astype(jnp.float32) + attn_total).astype(jnp.bfloat16)
    moe_normed = rms_scale(mixed_rows, moe_gain).astype(jnp.bfloat16)
    shared_gate_out = jnp.dot(moe_normed, shared_gate, preferred_element_type=jnp.float32)
    shared_up_out = jnp.dot(moe_normed, shared_up, preferred_element_type=jnp.float32)
    shared_hidden = (jax.nn.silu(shared_gate_out) * shared_up_out).astype(jnp.bfloat16)
    shared_part = jnp.dot(shared_hidden, shared_down, preferred_element_type=jnp.float32)
    experts = lax.axis_size("ep")
    top_count = expert_ids.shape[1]
    capacity = min(seq_dev, max(2, 2 * seq_dev * top_count // experts))
    slot_count = seq_dev * top_count
    slot_ids = expert_ids.reshape(slot_count)
    expert_hits = (slot_ids[:, None] == jnp.arange(experts, dtype=jnp.int32)[None, :]).astype(
        jnp.int32
    )
    slot_rank = jnp.sum((jnp.cumsum(expert_hits, axis=0) - expert_hits) * expert_hits, axis=1)
    slot_place = slot_ids * capacity + slot_rank
    placed = (
        slot_place[:, None] == jnp.arange(experts * capacity, dtype=jnp.int32)[None, :]
    ).astype(jnp.bfloat16)
    slot_token = jnp.arange(slot_count, dtype=jnp.int32) // top_count
    token_pick = (slot_token[:, None] == jnp.arange(seq_dev, dtype=jnp.int32)[None, :]).astype(
        jnp.bfloat16
    )
    dispatch = lax.dot_general(
        placed, token_pick, (((0,), (0,)), ((), ())), preferred_element_type=jnp.float32
    ).astype(jnp.bfloat16)
    col_count = model_width // lax.axis_size("tp")
    own_start = lax.axis_index("tp") * col_count
    own_normed = lax.dynamic_slice_in_dim(moe_normed, own_start, col_count, 1)
    send_slice = jnp.dot(dispatch, own_normed, preferred_element_type=jnp.float32).astype(
        jnp.bfloat16
    )
    arrived = lax.all_to_all(send_slice, "ep", split_axis=0, concat_axis=0, tiled=True)
    received = lax.all_gather(arrived, "tp", axis=1, tiled=True)
    gate_out = jnp.dot(received, gate_weight[0], preferred_element_type=jnp.float32)
    up_out = jnp.dot(received, up_weight[0], preferred_element_type=jnp.float32)
    expert_hidden = (jax.nn.silu(gate_out) * up_out).astype(jnp.bfloat16)
    expert_part = jnp.dot(expert_hidden, down_weight[0], preferred_element_type=jnp.float32)
    expert_sum, shared_out = scatter_sum(expert_part), scatter_sum(shared_part)
    returned = lax.all_to_all(
        expert_sum.astype(jnp.bfloat16), "ep", split_axis=0, concat_axis=0, tiled=True
    )
    slot_values = jnp.dot(placed, returned, preferred_element_type=jnp.float32).reshape(
        seq_dev, top_count, col_count
    )
    routed = jnp.sum(expert_weights[:, :, None] * slot_values, axis=1)
    own_cols = lax.dynamic_slice_in_dim(mixed_rows, own_start, col_count, 1)
    return (own_cols.astype(jnp.float32) + routed + shared_out).astype(jnp.bfloat16)


def solution(mesh):
    in_specs = (
        P("ep", None),
        P(),
        P(None, "tp"),
        P(None, "tp"),
        P(None, "tp"),
        P(None, "tp"),
        P("tp"),
        P(),
        P("ep", None, "tp", None),
        P("ep", None, "tp", None),
        P("ep"),
        P(),
        P("ep", None, "tp"),
        P("ep", None, "tp"),
        P("ep", "tp", None),
        P(None, "tp"),
        P(None, "tp"),
        P("tp", None),
        P("ep", None),
        P("ep", None),
    )
    out_specs = P("ep", "tp")
    return jax.shard_map(shards, mesh=mesh, in_specs=in_specs, out_specs=out_specs, check_vma=False)
```
